256 devices in a mesh: grp: 2 (over y), sp: 32 (over z, core), tp: 4 (over x).
Axes of the slice: x: 4, y: 2, z: 16, core: 2. Of those that a mesh axis runs over, the one named last changes fastest.
The devices are a block of a 4x16x16 slice.
Arguments:
- query_rows: bfloat16 [8192, 1024], P(('grp', 'sp'), 'tp'), parts along dimension 0, may hold values from -6 to 6
- key_rows: bfloat16 [8192, 1024], P(('grp', 'sp'), 'tp'), parts along dimension 0, may hold values from -6 to 6
- value_rows: bfloat16 [8192, 1024], P(('grp', 'sp'), 'tp'), parts along dimension 0, may hold values from -6 to 6
- gate_rows: bfloat16 [8192, 1024], P(('grp', 'sp'), 'tp'), parts along dimension 0, may hold values from -6 to 6
- log_decay: float32 [2, 8, 8192], P(None, 'tp', ('grp', 'sp')), parts along dimension 2, may hold values from -2 to 0, as said below
- head_gain: float32 [2, 1024], P(None, 'tp'), may hold values from 0.1 to 1.9
- out_weight: bfloat16 [1024, 2048], P('tp'), may hold values from -0.1875 to 0.1875
- residual: bfloat16 [8192, 2048], P(('grp', 'sp')), parts along dimension 0, may hold values from -6 to 6
- norm_gain: bfloat16 [2048], replicated, may hold values from 0.099609375 to 1.8984375
- gate_weight: bfloat16 [2048, 5632], P('sp', 'tp'), may hold values from -0.125 to 0.125
- up_weight: bfloat16 [2048, 5632], P('sp', 'tp'), may hold values from -0.125 to 0.125
- down_weight: bfloat16 [2048, 5632], P('sp', 'tp'), may hold values from -0.078125 to 0.078125
- gate_taps: bfloat16 [3, 5632], P(None, 'tp'), may hold values from -3.5 to 3.5
- up_taps: bfloat16 [3, 5632], P(None, 'tp'), may hold values from -3.5 to 3.5
Outputs:
- block_out: bfloat16 [8192, 2048], P(('grp', 'sp', 'tp')), parts along dimension 0
The draws below stay inside these ranges and needn't reach their ends.
There are 2 independent parts, one for each index of `grp`. The reference program is written for one: setup_inputs(seed, part) draws one part's arguments, and reference() takes and returns one part's arrays. A program takes and returns all parts, laid end to end along the dimension named above; an argument that names none is the same for every part. Nothing has to cross between parts.
Inputs may be any that keep to these rules, and one draw needn't show every extreme that they name: `log_decay`: every entry is negative.
All inputs are finite; a program needn't handle non-finite values.
Results may differ from the reference program's by a relative error of at most 0.017.
Values may be sent and summed in bfloat16 or wider, within the bound.
A program may use at most 64 MiB of HBM per device.

```python
import math
import jax
import jax.numpy as jnp
from jax import lax

D = 2048
RETENTION_HEADS = 8
HEAD = 128
FF = 5632
TOK_DEV = 128
VALUE = 1024
TOKENS = 4096


def spread_log(subkey, shape, low_end, high_end):
    return jnp.exp(jax.random.uniform(subkey, shape, jnp.float32, jnp.log(low_end), jnp.log(high_end)))


def draw_log_decay(key, part):
    random_subkeys = jax.random.split(jax.random.fold_in(key, 17), 7)
    blocks = TOKENS // TOK_DEV
    slow_share = 0.5
    totals = spread_log(random_subkeys[1], (2, RETENTION_HEADS, 1), 0.2, 0.7)
    is_slow = jax.random.bernoulli(random_subkeys[0], slow_share, (2, RETENTION_HEADS, 1))
    reach_len = spread_log(random_subkeys[2], (2, RETENTION_HEADS, 1), 30.0, 100.0)
    baseline_decay_rate = jnp.where(is_slow, -totals / TOKENS, -1.0 / reach_len)
    multiplier = spread_log(random_subkeys[3], (2, RETENTION_HEADS, blocks, 1), 0.5, 1.5)
    multiplier = jnp.broadcast_to(multiplier, (2, RETENTION_HEADS, blocks, TOK_DEV)).reshape(2, RETENTION_HEADS, TOKENS)
    approximate_multiplier = jax.random.uniform(random_subkeys[4], (2, RETENTION_HEADS, TOKENS), jnp.float32, 0.6, 1.4)
    target_locations = jax.random.randint(random_subkeys[5], (2, RETENTION_HEADS, 2, 1), 0, TOKENS)
    spike_depth = jnp.log(jax.random.uniform(random_subkeys[6], (2, RETENTION_HEADS, 2, 1), jnp.float32, 0.55, 0.8))
    token_positions = jnp.arange(TOKENS)[None, None, None, :]
    spike_events = jnp.sum(jnp.where(token_positions == target_locations, spike_depth, 0.0), axis=2)
    return (baseline_decay_rate * multiplier * approximate_multiplier + spike_events).astype(jnp.float32)


def block_levels(key, shape, pieces, low, high):
    level, own = 1.0, jax.random.fold_in(key, 6)
    for position, blocks in pieces:
        draws = jnp.exp(jax.random.uniform(jax.random.fold_in(own, position), (blocks,), jnp.float32, low / len(pieces), high / len(pieces)))
        level = level * jnp.repeat(draws, shape[position] // blocks).reshape([-1 if axis == position else 1 for axis in range(len(shape))])
    return level


def normal_values(key, extent, scale, bound, cuts=(), dtype=jnp.bfloat16):
    entries = jax.random.normal(key, extent, jnp.float32) * scale
    if len(cuts) > 0:
        entries = block_levels(key, extent, cuts, -0.22, 0.18) * entries
    return jnp.clip(entries, min=-bound, max=bound).astype(dtype)


def setup_inputs(seed: int = 0, part: int = 0) -> dict:
    splits = jax.random.split(jax.random.key(seed), 15)
    part_keys = jax.random.split(jax.random.fold_in(splits[14], part), 15)
    query_rows = normal_values(part_keys[0], (TOKENS, VALUE), 1.0, 6.0, ((0, 32), (1, 4)))
    key_rows = normal_values(part_keys[1], (TOKENS, VALUE), 1.0, 6.0, ((0, 32), (1, 4)))
    value_rows = normal_values(part_keys[2], (TOKENS, VALUE), 1.0, 6.0, ((0, 32), (1, 4)))
    gate_rows = normal_values(part_keys[3], (TOKENS, VALUE), 1.0, 6.0, ((0, 32), (1, 4)))
    log_decay = draw_log_decay(jax.random.fold_in(jax.random.fold_in(splits[14], part), 71), part)
    head_gain = jnp.clip(1.0 + 0.18 * jax.random.normal(splits[5], (2, VALUE), jnp.float32), 0.1, 1.9)
    out_weight = normal_values(splits[6], (VALUE, D), VALUE ** -0.5, 0.1875, ((0, 4),))
    residual = normal_values(part_keys[7], (TOKENS, D), 1.0, 6.0, ((0, 32),))
    norm_gain = jnp.clip(1.0 + 0.18 * jax.random.normal(splits[8], (D,), jnp.float32), 0.099609375, 1.8984375).astype(jnp.bfloat16)
    gate_weight = normal_values(splits[9], (D, FF), D ** -0.5, 0.125, ((0, 32), (1, 4)))
    up_weight = normal_values(splits[10], (D, FF), D ** -0.5, 0.125, ((0, 32), (1, 4)))
    down_weight = normal_values(splits[11], (D, FF), FF ** -0.5, 0.078125, ((0, 32), (1, 4)))
    gate_taps = normal_values(splits[12], (3, FF), 3 ** -0.5, 3.5, ((1, 4),))
    up_taps = normal_values(splits[13], (3, FF), 3 ** -0.5, 3.5, ((1, 4),))
    return {"query_rows": query_rows, "key_rows": key_rows, "value_rows": value_rows, "gate_rows": gate_rows, "log_decay": log_decay, "head_gain": head_gain, "out_weight": out_weight, "residual": residual, "norm_gain": norm_gain, "gate_weight": gate_weight, "up_weight": up_weight, "down_weight": down_weight, "gate_taps": gate_taps, "up_taps": up_taps}


FULL_PRECISION = lax.Precision.HIGHEST
GROUP_EPS = 1e-05
NORM_EPS = 1e-06

def scan_retention(query_all, key_all, value_all, log_rates):
    length, head_count, head_width = query_all.shape
    block_len = math.gcd(length, 512)
    block_count = length // block_len
    query_blocks = query_all.reshape(block_count, block_len, head_count, head_width)
    key_blocks = key_all.reshape(block_count, block_len, head_count, head_width)
    value_blocks = value_all.reshape(block_count, block_len, head_count, head_width)
    rate_blocks = log_rates.T.reshape(block_count, block_len, head_count)
    lower_mask = jnp.arange(block_len)[:, None] >= jnp.arange(block_len)[None, :]

    def block_step(carry_state, inputs):
        query_blk, key_blk, value_blk, rate_blk = inputs
        cumul = jnp.cumsum(rate_blk, axis=0)
        gap_logs = cumul[:, None, :] - cumul[None, :, :]
        decay_mask = jnp.where(lower_mask[:, :, None], jnp.exp(jnp.minimum(gap_logs, 0.0)), 0.0)
        scores = jnp.einsum('thd,shd->tsh', query_blk, key_blk, precision=FULL_PRECISION) * decay_mask
        inner_part = jnp.einsum('tsh,she->the', scores, value_blk, precision=FULL_PRECISION)
        carried = jnp.einsum('thd,hde->the', query_blk * jnp.exp(cumul)[:, :, None], carry_state, precision=FULL_PRECISION)
        last_cumul = cumul[-1]
        key_decayed = key_blk * jnp.exp(last_cumul[None, :] - cumul)[:, :, None]
        new_state = carry_state * jnp.exp(last_cumul)[:, None, None] + jnp.einsum('shd,she->hde', key_decayed, value_blk, precision=FULL_PRECISION)
        return (new_state, inner_part + carried)
    zero_state = jnp.zeros((head_count, head_width, head_width), jnp.float32)
    ignored, block_outs = lax.scan(block_step, zero_state, (query_blocks, key_blocks, value_blocks, rate_blocks))
    return block_outs.reshape(length, head_count, head_width)

def group_norm(values):
    length, head_count, head_width = values.shape
    centre = values - lax.optimization_barrier(jnp.mean(values, axis=2, keepdims=True))
    spread = lax.optimization_barrier(jnp.mean(centre * centre, axis=2, keepdims=True))
    return (centre * lax.rsqrt(spread + GROUP_EPS)).reshape(length, head_count * head_width)

def rms_scale(middle, gain):
    values = middle.astype(jnp.float32)
    multiplier = lax.rsqrt(lax.optimization_barrier(jnp.mean(values * values, axis=1, keepdims=True)) + NORM_EPS)
    return (values * multiplier * gain.astype(jnp.float32)).astype(jnp.bfloat16)

def reference(query_rows, key_rows, value_rows, gate_rows, log_decay, head_gain, out_weight, residual, norm_gain, gate_weight, up_weight, down_weight, gate_taps, up_taps):
    key_scale = HEAD ** (-0.5)
    query_all = query_rows.astype(jnp.float32).reshape(TOKENS, RETENTION_HEADS, HEAD)
    key_all = key_rows.astype(jnp.float32).reshape(TOKENS, RETENTION_HEADS, HEAD) * key_scale
    value_all = value_rows.astype(jnp.float32).reshape(TOKENS, RETENTION_HEADS, HEAD)
    ahead_out = scan_retention(query_all, key_all, value_all, log_decay[0])
    behind_out = scan_retention(query_all[::-1], key_all[::-1], value_all[::-1], log_decay[1][:, ::-1])[::-1]
    combined = group_norm(ahead_out) * head_gain[0] + group_norm(behind_out) * head_gain[1]
    mixed_heads = (jax.nn.silu(gate_rows.astype(jnp.float32)) * combined).astype(jnp.bfloat16)
    attended = jnp.dot(mixed_heads, out_weight, preferred_element_type=jnp.float32)
    middle = lax.optimization_barrier((residual.astype(jnp.float32) + attended).astype(jnp.bfloat16))
    normed = rms_scale(middle, norm_gain)
    model_width = normed.shape[1]
    zero_row = jnp.zeros((1, model_width), jnp.bfloat16)
    padded = jnp.concatenate([zero_row, normed, zero_row], axis=0)
    block_len = math.gcd(TOKENS, 512)
    taps_gate = gate_taps.astype(jnp.float32)
    taps_up = up_taps.astype(jnp.float32)

    def one_block(block_index):
        first_row = (block_index * block_len).astype(jnp.int32)
        rows_with_rims = lax.dynamic_slice_in_dim(padded, first_row, block_len + 2, 0)
        pre_gate = lax.optimization_barrier(jnp.dot(rows_with_rims, gate_weight, preferred_element_type=jnp.float32).astype(jnp.bfloat16)).astype(jnp.float32)
        pre_up = lax.optimization_barrier(jnp.dot(rows_with_rims, up_weight, preferred_element_type=jnp.float32).astype(jnp.bfloat16)).astype(jnp.float32)
        conv_gate = taps_gate[0] * pre_gate[:-2] + taps_gate[1] * pre_gate[1:-1] + taps_gate[2] * pre_gate[2:]
        conv_up = taps_up[0] * pre_up[:-2] + taps_up[1] * pre_up[1:-1] + taps_up[2] * pre_up[2:]
        hidden = (jax.nn.silu(conv_gate) * conv_up).astype(jnp.bfloat16)
        ff_out = lax.dot_general(hidden, down_weight, (((1,), (1,)), ((), ())), preferred_element_type=jnp.float32)
        middle_rows = lax.dynamic_slice_in_dim(middle, first_row, block_len, 0).astype(jnp.float32)
        return (middle_rows + ff_out).astype(jnp.bfloat16)
    block_outs = lax.map(one_block, jnp.arange(TOKENS // block_len).astype(jnp.int32))
    return block_outs.reshape(TOKENS, model_width)
```

```python
import functools

import jax
import jax.numpy as jnp
from jax import lax
from jax.experimental import pallas as pl
from jax.experimental.pallas import tpu as pltpu
from jax.sharding import PartitionSpec as P

HEAD = 128
LANE = 128
GROUP_EPS = 1e-05
NORM_EPS = 1e-06
MESH = pl.DeviceIdType.MESH
F32 = jnp.float32
BF16 = jnp.bfloat16


def nt(a, b):
    return lax.dot_general(a, b, (((1,), (1,)), ((), ())), preferred_element_type=F32)


def tn(a, b):
    return lax.dot_general(a, b, (((0,), (0,)), ((), ())), preferred_element_type=F32)


def nn(a, b):
    return jnp.dot(a, b, preferred_element_type=F32)


class Place:
    def __init__(self, groups, spans, peers):
        self.spans, self.peers, self.chips = spans, peers, spans // 2
        self.sp = lax.axis_index("sp")
        self.tp = lax.axis_index("tp")
        self.core = lax.rem(self.sp, 2)
        self.z = lax.div(self.sp, 2)
        self.paired = groups % 2 == 0
        grp = lax.axis_index("grp")
        self.side = lax.rem(grp, 2)
        self.pair = {"grp": grp + 1 - 2 * self.side}
        self.twin = {"sp": self.sp + 1 - 2 * self.core}

    def chip(self, step):
        return lax.rem(self.z + step + self.chips, self.chips)

    def along(self, step):
        return {"sp": 2 * self.chip(step) + self.core}

    def span(self, step):
        return lax.rem(self.sp + step + self.spans, self.spans)

    def peer(self, step):
        return lax.rem(self.tp + step, self.peers)

    def slot_chip(self, slot):
        step = (slot + 1) // 2
        return self.chip(-step if slot % 2 else step)


def remote(src, dst, send_sem, recv_sem, device):
    return pltpu.make_async_remote_copy(
        src_ref=src, dst_ref=dst, send_sem=send_sem, recv_sem=recv_sem, device_id=device, device_id_type=MESH
    )


class Stream:
    def __init__(self, place, buf, halves, sems):
        self.p, self.buf, self.halves = place, buf, halves
        self.ring_s, self.ring_r, self.pair_s, self.pair_r, self.twin_s, self.twin_r, self.twin2_s, self.twin2_r = sems
        width = buf.shape[1]
        tiles = width // LANE
        ring = round(2 * tiles / 3) if place.paired else tiles
        self.width = width
        self.ring_w = ring * LANE
        self.pair_w = width - self.ring_w
        self.ring_o = pl.multiple_of(place.side * self.pair_w, LANE) if place.paired else 0
        self.pair_o = pl.multiple_of((1 - place.side) * self.ring_w, LANE)
        self.give_o = pl.multiple_of(place.side * self.ring_w, LANE)
        self.block = buf.shape[0] // place.spans
        self.rows = self.block // halves
        self.last = place.chips // 2
        self.opposite = place.chips - 1
        self.started = []
        self.handed = {0}

    def view(self, slot, half, cols, core=None):
        core = self.p.core if core is None else core
        start = pl.multiple_of(slot * 2 * self.block + core * self.block + half * self.rows, self.rows)
        return self.buf.at[pl.ds(start, self.rows), cols]

    def ring_cols(self):
        return pl.ds(self.ring_o, self.ring_w)

    def send(self, src, dst, s, r, device):
        copy = remote(src, dst, s, r, device)
        copy.start()
        self.started.append(copy)

    def to_twin(self, slot, half, cols, s, r):
        view = self.view(slot, half, cols)
        self.send(view, view, s.at[slot, half], r.at[slot, half], self.p.twin)

    def to_pair(self, slot, half):
        if self.p.paired:
            view = self.view(slot, half, pl.ds(self.give_o, self.pair_w))
            self.send(view, view, self.pair_s.at[slot, half], self.pair_r.at[slot, half], self.p.pair)

    def own(self, half):
        cols = self.ring_cols()
        src = self.view(0, half, cols)
        self.send(src, self.view(1, half, cols), self.ring_s.at[0, half], self.ring_r.at[1, half], self.p.along(1))
        self.send(
            src, self.view(2, half, cols), self.ring_s.at[self.opposite, half], self.ring_r.at[2, half], self.p.along(-1)
        )
        self.to_twin(0, half, pl.ds(0, self.width), self.twin_s, self.twin_r)

    def got(self, slot, half):
        view = self.view(slot, half, self.ring_cols())
        remote(view, view, self.ring_s.at[slot, half], self.ring_r.at[slot, half], self.p.along(1)).wait_recv()

    def tick(self, step, half):
        cols = self.ring_cols()
        if step == self.last:
            slots = (self.opposite,)
            self.got(self.opposite, half)
        else:
            behind, ahead = slots = (2 * step - 1, 2 * step)
            if step + 1 < self.last:
                for slot, way in ((behind, 1), (ahead, -1)):
                    self.got(slot, half)
                    self.send(
                        self.view(slot, half, cols),
                        self.view(slot + 2, half, cols),
                        self.ring_s.at[slot, half],
                        self.ring_r.at[slot + 2, half],
                        self.p.along(way),
                    )
            else:
                self.got(behind, half)
                self.got(ahead, half)
                slot = behind + self.p.core
                self.send(
                    self.view(slot, half, cols),
                    self.view(self.opposite, half, cols),
                    self.ring_s.at[slot, half],
                    self.ring_r.at[self.opposite, half],
                    self.p.along(1 - 2 * self.p.core),
                )
        for slot in slots:
            self.to_pair(slot, half)
            self.to_twin(slot, half, cols, self.twin_s, self.twin_r)

    def pair_tick(self, step, half):
        slots = (self.opposite,) if step == self.last else (2 * step - 1, 2 * step)
        if half == self.halves - 1:
            self.handed.update(slots)
        if not self.p.paired:
            return
        cols = pl.ds(self.pair_o, self.pair_w)
        for slot in slots:
            view = self.view(slot, half, cols)
            remote(view, view, self.pair_s.at[slot, half], self.pair_r.at[slot, half], self.p.pair).wait_recv()
            self.to_twin(slot, half, cols, self.twin2_s, self.twin2_r)

    def ready(self, slot):
        for half in range(self.halves):
            cols = pl.ds(0, self.width) if slot == 0 else self.ring_cols()
            view = self.view(slot, half, cols, 1 - self.p.core)
            remote(view, view, self.twin_s.at[slot, half], self.twin_r.at[slot, half], self.p.twin).wait_recv()
            if self.p.paired and slot > 0:
                view = self.view(slot, half, pl.ds(self.pair_o, self.pair_w), 1 - self.p.core)
                remote(view, view, self.twin2_s.at[slot, half], self.twin2_r.at[slot, half], self.p.twin).wait_recv()

    def drain(self):
        for copy in self.started:
            copy.wait_send()


def order(gate_up, down, last, lag):
    late = []

    def one(stream, step, half):
        stream.tick(step, half)
        late.append((stream, step, half))

    for step in range(1, last + lag + 1):
        for half in range(gate_up.halves):
            if step <= last:
                while len(late) > 1:
                    a, b, c = late.pop(0)
                    a.pair_tick(b, c)
                one(gate_up, step, half)
                yield
        for half in range(down.halves):
            if step == lag:
                down.own(half)
            elif step > lag:
                while len(late) > 1:
                    a, b, c = late.pop(0)
                    a.pair_tick(b, c)
                one(down, step - lag, half)
                yield
    for a, b, c in late:
        a.pair_tick(b, c)


def all_to_all(place, src, dst, send_sem, recv_sem):
    spans = place.spans

    def body(t, _):
        step = spans // 2 + (1 - 2 * lax.rem(t, 2)) * lax.div(t + 1, 2)
        to = lax.rem(place.sp + step, spans)
        for s, d, ss, rs in zip(src(to), dst(place.sp), send_sem, recv_sem):
            remote(s, d, ss, rs, {"sp": to}).start()
        return 0

    lax.fori_loop(0, spans - 1, body, 0)


def wait_bytes(view, sem):
    pltpu.make_async_copy(view, view, sem).wait()


def layer(
    groups, spans, peers,
    q_ref, k_ref, v_ref, g_ref, ld_ref, hg_ref, wo_hbm, res_hbm, ng_ref, gw_hbm, uw_hbm, dw_hbm, gt_ref, ut_ref,
    out_ref,
    gu, dn, wo, res, st_send, st_recv, dec_send, dec_recv, in_send, in_recv, inner, grow, mix, att, att_r,
    mid, nsend, nall, nperm, pre, halo_s, halo_r, hid, ff, ff_r,
    load_sem, a2a_s, a2a_r, rs1_s, rs1_r, ag_s, ag_r, halo_ss, halo_rs, rs2_s, rs2_r,
    g0, g1, g2, g3, g4, g5, g6, g7, d0, d1, d2, d3, d4, d5, d6, d7,
):
    place = Place(groups, spans, peers)
    sp, tp, core = place.sp, place.tp, place.core
    length = q_ref.shape[0]
    heads = q_ref.shape[1] // HEAD
    combos = 2 * heads
    share = length // peers
    half_w = gw_hbm.shape[1]
    block = gw_hbm.shape[0]
    slots = place.chips
    scale = HEAD ** (-0.5)

    barrier = pltpu.get_barrier_semaphore()

    def greet(step, _):
        pl.semaphore_signal(barrier, inc=1, device_id={"sp": place.span(step)}, device_id_type=MESH)
        return 0

    pl.semaphore_signal(barrier, inc=1, device_id=place.along(1), device_id_type=MESH)
    pl.semaphore_signal(barrier, inc=1, device_id=place.along(-1), device_id_type=MESH)
    lax.fori_loop(3, spans - 2, greet, 0)
    for step in (1, 2 * 0 + spans - 1):
        pl.semaphore_signal(barrier, inc=1, device_id={"sp": place.span(step)}, device_id_type=MESH)
    greeted = spans - 1
    for step in range(1, peers):
        pl.semaphore_signal(barrier, inc=1, device_id={"tp": place.peer(step)}, device_id_type=MESH)
    greeted += peers - 1
    if place.paired:
        pl.semaphore_signal(barrier, inc=1, device_id=place.pair, device_id_type=MESH)
        greeted += 1

    own_rows = pl.ds(pl.multiple_of(core * block, block), block)
    loads = [
        pltpu.make_async_copy(gw_hbm, gu.at[own_rows, pl.ds(0, half_w)], load_sem.at[0]),
        pltpu.make_async_copy(uw_hbm, gu.at[own_rows, pl.ds(half_w, half_w)], load_sem.at[1]),
        pltpu.make_async_copy(dw_hbm, dn.at[own_rows, :], load_sem.at[2]),
        pltpu.make_async_copy(wo_hbm, wo, load_sem.at[3]),
        pltpu.make_async_copy(res_hbm.at[pl.ds(pl.multiple_of(tp * share, share), share), :], res, load_sem.at[4]),
    ]
    for copy in loads:
        copy.start()

    row = lax.broadcasted_iota(jnp.int32, (HEAD, LANE), 0)
    lane = lax.broadcasted_iota(jnp.int32, (HEAD, LANE), 1)
    rates = [ld_ref[d, pl.ds(h, 1), :] for h in range(heads) for d in range(2)]
    sums = jnp.concatenate(rates + rates[: (-combos) % 8], axis=0) if combos % 8 else jnp.concatenate(rates, axis=0)
    s_lane = lax.broadcasted_iota(jnp.int32, sums.shape, 1)
    s_row = lax.broadcasted_iota(jnp.int32, sums.shape, 0)
    back = (s_row & 1) == 1
    shift = 1
    while shift < length:
        fwd = jnp.where(s_lane >= shift, pltpu.roll(sums, shift, 1), 0.0)
        bwd = jnp.where(s_lane < length - shift, pltpu.roll(sums, length - shift, 1), 0.0)
        sums = sums + jnp.where(back, bwd, fwd)
        shift *= 2
    part = spans // combos
    rows = HEAD // part
    for h in range(heads):
        cols = pl.ds(h * HEAD, HEAD)
        q, k, v = q_ref[:, cols], k_ref[:, cols], v_ref[:, cols]
        v32 = v.astype(F32)
        scores = nt(q, k) * scale
        for d in range(2):
            m = 2 * h + d
            along_s = jnp.broadcast_to(sums[m : m + 1, :], (length, LANE))
            along_t = along_s.T
            seen = (row >= lane) if d == 0 else (row <= lane)
            decay = jnp.where(seen, jnp.exp(jnp.minimum(along_t - along_s, 0.0)), 0.0)
            inner[m] = nn((scores * decay).astype(BF16), v)
            grow[m] = jnp.exp(along_t) * scale
            total = along_t[length - 1 : length, :] if d == 0 else along_t[0:1, :]
            dec_send[m] = jnp.exp(total)
            faded = (v32 * jnp.exp(jnp.minimum(total - along_t, 0.0))).astype(BF16)
            st_send[pl.ds(m * part, part)] = tn(k, faded).astype(BF16).reshape(part, rows, HEAD)

    gate_up = Stream(place, gu, 2, (g0, g1, g2, g3, g4, g5, g6, g7))
    down = Stream(place, dn, 2, (d0, d1, d2, d3, d4, d5, d6, d7))
    ring = order(gate_up, down, place.chips // 2, 2)

    def advance(n):
        for _ in range(n):
            next(ring, None)

    def ready(stream, first, end):
        for slot in range(first, end):
            while slot not in stream.handed:
                next(ring, None)
            stream.ready(slot)

    for copy in loads[:3]:
        copy.wait()
    pl.semaphore_wait(barrier, greeted)

    all_to_all(
        place,
        lambda to: (st_send.at[to], dec_send.at[lax.div(to, part)]),
        lambda me: (st_recv.at[me], dec_recv.at[me]),
        (a2a_s.at[0], a2a_s.at[1]),
        (a2a_r.at[0], a2a_r.at[1]),
    )
    gate_up.own(0)
    gate_up.own(1)
    my_combo = lax.div(sp, part)
    st_recv[pl.ds(sp, 1)] = st_send[pl.ds(sp, 1)]
    dec_recv[pl.ds(sp, 1)] = dec_send[pl.ds(my_combo, 1)]
    advance(ADVANCE[0])
    others = pl.ds(0, spans - 1)
    wait_bytes(st_recv.at[others], a2a_r.at[0])
    wait_bytes(dec_recv.at[others], a2a_r.at[1])

    reverse = lax.rem(my_combo, 2)

    def scan(j, carry):
        at = j + reverse * (spans - 1 - 2 * j)
        in_send[at] = carry.astype(BF16)
        return carry * dec_recv[at] + st_recv[at].astype(F32)

    lax.fori_loop(0, spans, scan, jnp.zeros((rows, HEAD), F32))
    all_to_all(
        place, lambda to: (in_send.at[to],), lambda me: (in_recv.at[me],), (a2a_s.at[2],), (a2a_r.at[2],)
    )
    in_recv[pl.ds(sp, 1)] = in_send[pl.ds(sp, 1)]
    advance(ADVANCE[1])
    for copy in loads[3:]:
        copy.wait()
    wait_bytes(in_recv.at[others], a2a_r.at[2])

    def normed_head(x):
        centre = x - jnp.mean(x, axis=1, keepdims=True)
        spread = jnp.mean(centre * centre, axis=1, keepdims=True)
        return centre * lax.rsqrt(spread + GROUP_EPS)

    for h in range(heads):
        cols = pl.ds(h * HEAD, HEAD)
        q = q_ref[:, cols]
        combined = None
        for d in range(2):
            m = 2 * h + d
            state = in_recv[pl.ds(m * part, part)].reshape(HEAD, HEAD)
            term = normed_head(inner[m] + grow[m] * nn(q, state)) * hg_ref[pl.ds(d, 1), cols]
            combined = term if combined is None else combined + term
        gate = g_ref[:, cols].astype(F32)
        mix[:, cols] = (gate / (1.0 + jnp.exp(-gate)) * combined).astype(BF16)

    width = wo.shape[1]
    tile = min(512, width)
    for n in range(width // tile):
        cols = pl.ds(n * tile, tile)
        att[:, cols] = nn(mix[...], wo[:, cols]).astype(BF16)

    def peer_rows(j):
        return pl.ds(pl.multiple_of(j * share, share), share)

    started = []

    def to_peers(src, dst, s, r):
        for step in range(1, peers):
            copy = remote(src(place.peer(step)), dst(step), s.at[step - 1], r.at[step - 1], {"tp": place.peer(step)})
            copy.start()
            started.append(copy)

    to_peers(lambda j: att.at[peer_rows(j), :], lambda step: att_r.at[step - 1], rs1_s, rs1_r)
    advance(ADVANCE[2])
    for step in range(1, peers):
        remote(att_r.at[step - 1], att_r.at[step - 1], rs1_s.at[step - 1], rs1_r.at[step - 1], {"tp": tp}).wait_recv()
    total = att[peer_rows(tp), :].astype(F32)
    for step in range(1, peers):
        total = total + att_r[step - 1].astype(F32)
    middle = (res[...].astype(F32) + total).astype(BF16)
    mid[...] = middle
    values = middle.astype(F32)
    multiplier = lax.rsqrt(jnp.mean(values * values, axis=1, keepdims=True) + NORM_EPS)
    normed = (values * multiplier * ng_ref[...].astype(F32)).astype(BF16)
    nsend[...] = normed
    nall[peer_rows(tp), :] = normed
    to_peers(lambda j: nsend, lambda step: nall.at[peer_rows(tp), :], ag_s, ag_r)
    advance(ADVANCE[3])
    for step in range(1, peers):
        view = nall.at[peer_rows(place.peer(peers - step)), :]
        remote(view, view, ag_s.at[step - 1], ag_r.at[step - 1], {"tp": tp}).wait_recv()
    for slot in range(slots):
        start = pl.multiple_of(place.slot_chip(slot) * LANE, LANE)
        nperm[:, pl.ds(slot * LANE, LANE)] = nall[:, pl.ds(start, LANE)]

    advance(ADVANCE[4])
    ready(gate_up, 0, slots)

    n_tile = 256 if (2 * half_w) % 256 == 0 else 128

    def project(n, _):
        cols = pl.ds(pl.multiple_of(n * n_tile, n_tile), n_tile)
        pre[:, cols] = nn(nperm[...], gu[:, cols]).astype(BF16).astype(F32)
        return 0

    lax.fori_loop(0, 2 * half_w // n_tile, project, 0)
    halo_s[0] = pre[0:1, :]
    halo_s[1] = pre[length - 1 : length, :]
    before, after = {"sp": place.span(-1)}, {"sp": place.span(1)}
    halos = [
        remote(halo_s.at[0], halo_r.at[1], halo_ss.at[0], halo_rs.at[1], before),
        remote(halo_s.at[1], halo_r.at[0], halo_ss.at[1], halo_rs.at[0], after),
    ]
    for copy in halos:
        copy.start()
    advance(ADVANCE[5])
    for copy in halos:
        copy.wait_recv()
    not_first = (sp > 0).astype(F32)
    not_last = (sp < spans - 1).astype(F32)

    def conv(n, _):
        results = []
        for base, taps in ((0, gt_ref), (half_w, ut_ref)):
            cols = pl.ds(pl.multiple_of(base + n * LANE, LANE), LANE)
            x = pre[:, cols]
            above = jnp.where(row == 0, halo_r[0, :, cols] * not_first, pltpu.roll(x, 1, 0))
            below = jnp.where(row == length - 1, halo_r[1, :, cols] * not_last, pltpu.roll(x, length - 1, 0))
            t = taps[:, pl.ds(pl.multiple_of(n * LANE, LANE), LANE)].astype(F32)
            results.append(t[0:1] * above + t[1:2] * x + t[2:3] * below)
        gate, up = results
        hid[:, pl.ds(pl.multiple_of(n * LANE, LANE), LANE)] = (gate / (1.0 + jnp.exp(-gate)) * up).astype(BF16)
        return 0

    lax.fori_loop(0, half_w // LANE, conv, 0)

    cut = slots // 2
    for part_no, (lo, hi) in enumerate(((0, cut), (cut, slots))):
        ready(down, lo, hi)

        def project_down(n, _):
            rows_ = pl.ds(pl.multiple_of(n * 2 * LANE, 2 * LANE), 2 * LANE)
            ff[:, rows_] = nt(hid[...], dn[rows_, :]).astype(BF16)
            return 0

        lax.fori_loop(lo // 2, hi // 2, project_down, 0)
        cols = pl.ds(lo * LANE, (hi - lo) * LANE)
        to_peers(
            lambda j: ff.at[peer_rows(j), cols],
            lambda step: ff_r.at[step - 1, :, cols],
            rs2_s.at[part_no],
            rs2_r.at[part_no],
        )
    for part_no, (lo, hi) in enumerate(((0, cut), (cut, slots))):
        cols = pl.ds(lo * LANE, (hi - lo) * LANE)
        for step in range(1, peers):
            view = ff_r.at[step - 1, :, cols]
            remote(view, view, rs2_s.at[part_no, step - 1], rs2_r.at[part_no, step - 1], {"tp": tp}).wait_recv()
        for slot in range(lo, hi):
            held = pl.ds(slot * LANE, LANE)
            home = pl.ds(pl.multiple_of(place.slot_chip(slot) * LANE, LANE), LANE)
            total = ff[peer_rows(tp), held].astype(F32)
            for step in range(1, peers):
                total = total + ff_r[step - 1, :, held].astype(F32)
            out_ref[:, home] = (mid[:, home].astype(F32) + total).astype(BF16)

    advance(10_000)
    for copy in started + halos:
        copy.wait_send()
    wait_bytes(st_send.at[others], a2a_s.at[0])
    wait_bytes(dec_recv.at[others], a2a_s.at[1])
    wait_bytes(in_send.at[others], a2a_s.at[2])
    gate_up.drain()
    down.drain()


ADVANCE = (3, 3, 4, 5, 10, 3)


def solution(mesh):
    groups, spans, peers = mesh.shape["grp"], mesh.shape["sp"], mesh.shape["tp"]
    rows_, cols_ = ("grp", "sp"), "tp"
    placed = (
        P(rows_, cols_), P(rows_, cols_), P(rows_, cols_), P(rows_, cols_), P(None, cols_, rows_), P(None, cols_),
        P(cols_, None), P(rows_, None), P(), P("sp", cols_), P("sp", cols_), P("sp", cols_), P(None, cols_),
        P(None, cols_),
    )

    def shards(q, k, v, g, ld, hg, wo, res, ng, gw, uw, dw, gt, ut):
        length = q.shape[0]
        heads = q.shape[1] // HEAD
        combos = 2 * heads
        share = length // peers
        block, half_w = gw.shape
        width = wo.shape[1]
        chips = spans // 2
        packet = HEAD * combos // spans
        dma = pltpu.SemaphoreType.DMA
        vmem = pl.BlockSpec(memory_space=pltpu.VMEM)
        any_ = pl.BlockSpec(memory_space=pl.ANY)
        scratch = [
            pltpu.VMEM((spans * block, 2 * half_w), BF16),
            pltpu.VMEM((spans * block, half_w), BF16),
            pltpu.VMEM(wo.shape, BF16),
            pltpu.VMEM((share, width), BF16),
            pltpu.VMEM((spans, packet, HEAD), BF16),
            pltpu.VMEM((spans, packet, HEAD), BF16),
            pltpu.VMEM((combos, 1, LANE), F32),
            pltpu.VMEM((spans, 1, LANE), F32),
            pltpu.VMEM((spans, packet, HEAD), BF16),
            pltpu.VMEM((spans, packet, HEAD), BF16),
            pltpu.VMEM((combos, length, HEAD), F32),
            pltpu.VMEM((combos, length, HEAD), F32),
            pltpu.VMEM((length, heads * HEAD), BF16),
            pltpu.VMEM((length, width), BF16),
            pltpu.VMEM((peers - 1, share, width), BF16),
            pltpu.VMEM((share, width), BF16),
            pltpu.VMEM((share, width), BF16),
            pltpu.VMEM((length, width), BF16),
            pltpu.VMEM((length, width), BF16),
            pltpu.VMEM((length, 2 * half_w), F32),
            pltpu.VMEM((2, 1, 2 * half_w), F32),
            pltpu.VMEM((2, 1, 2 * half_w), F32),
            pltpu.VMEM((length, half_w), BF16),
            pltpu.VMEM((length, width), BF16),
            pltpu.VMEM((peers - 1, share, width), BF16),
            dma((5,)), dma((3,)), dma((3,)), dma((peers - 1,)), dma((peers - 1,)), dma((peers - 1,)), dma((peers - 1,)),
            dma((2,)), dma((2,)), dma((2, peers - 1)), dma((2, peers - 1)),
        ] + [dma((chips, 2)) for _ in range(16)]
        return pl.pallas_call(
            functools.partial(layer, groups, spans, peers),
            name="layer",
            out_shape=jax.ShapeDtypeStruct((share, width), BF16),
            in_specs=[vmem] * 6 + [any_, any_, vmem, any_, any_, any_, vmem, vmem],
            out_specs=vmem,
            scratch_shapes=scratch,
            compiler_params=pltpu.CompilerParams(
                collective_id=0, has_side_effects=True, vmem_limit_bytes=50 * 1024 * 1024
            ),
        )(q, k, v, g, ld, hg, wo, res, ng.reshape(1, -1), gw, uw, dw, gt, ut)

    return jax.shard_map(shards, mesh=mesh, in_specs=placed, out_specs=P(("grp", "sp", "tp"), None), check_vma=False)
```

```python
import functools

import jax
import jax.numpy as jnp
from jax import lax
from jax.experimental import pallas as pl
from jax.experimental.pallas import tpu as pltpu
from jax.sharding import PartitionSpec as P

HEAD = 128
LANE = 128
GROUP_EPS = 1e-05
NORM_EPS = 1e-06
MESH = pl.DeviceIdType.MESH
F32 = jnp.float32
BF16 = jnp.bfloat16


def nt(a, b):
    return lax.dot_general(a, b, (((1,), (1,)), ((), ())), preferred_element_type=F32)


def tn(a, b):
    return lax.dot_general(a, b, (((0,), (0,)), ((), ())), preferred_element_type=F32)


def nn(a, b):
    return jnp.dot(a, b, preferred_element_type=F32)


class Place:
    def __init__(self, groups, spans, peers):
        self.spans, self.peers, self.chips = spans, peers, spans // 2
        self.sp = lax.axis_index("sp")
        self.tp = lax.axis_index("tp")
        self.core = lax.rem(self.sp, 2)
        self.z = lax.div(self.sp, 2)
        self.paired = PAIRED and groups % 2 == 0
        grp = lax.axis_index("grp")
        self.side = lax.rem(grp, 2)
        self.pair = {"grp": grp + 1 - 2 * self.side}
        self.twin = {"sp": self.sp + 1 - 2 * self.core}

    def chip(self, step):
        return lax.rem(self.z + step + self.chips, self.chips)

    def along(self, step):
        return {"sp": 2 * self.chip(step) + self.core}

    def span(self, step):
        return lax.rem(self.sp + step + self.spans, self.spans)

    def peer(self, step):
        return lax.rem(self.tp + step, self.peers)

    def slot_chip(self, slot):
        step = (slot + 1) // 2
        return self.chip(-step if slot % 2 else step)


def remote(src, dst, send_sem, recv_sem, device):
    return pltpu.make_async_remote_copy(
        src_ref=src, dst_ref=dst, send_sem=send_sem, recv_sem=recv_sem, device_id=device, device_id_type=MESH
    )


class Stream:
    def __init__(self, place, buf, halves, sems):
        self.p, self.buf, self.halves = place, buf, halves
        self.ring_s, self.ring_r, self.pair_s, self.pair_r, self.twin_s, self.twin_r, self.twin2_s, self.twin2_r = sems
        width = buf.shape[1]
        tiles = width // LANE
        ring = max((tiles + 1) // 2, int(RING_SHARE * tiles)) if place.paired else tiles
        self.width = width
        self.ring_w = ring * LANE
        self.pair_w = width - self.ring_w
        self.ring_o = pl.multiple_of(place.side * self.pair_w, LANE) if place.paired else 0
        self.pair_o = pl.multiple_of((1 - place.side) * self.ring_w, LANE)
        self.give_o = pl.multiple_of(place.side * self.ring_w, LANE)
        self.block = buf.shape[0] // place.spans
        self.rows = self.block // halves
        self.last = place.chips // 2
        self.opposite = place.chips - 1
        self.started = []
        self.handed = {0}

    def view(self, slot, half, cols, core=None):
        core = self.p.core if core is None else core
        start = pl.multiple_of(slot * 2 * self.block + core * self.block + half * self.rows, self.rows)
        return self.buf.at[pl.ds(start, self.rows), cols]

    def ring_cols(self):
        return pl.ds(self.ring_o, self.ring_w)

    def send(self, src, dst, s, r, device):
        copy = remote(src, dst, s, r, device)
        copy.start()
        self.started.append(copy)

    def to_twin(self, slot, half, cols, s, r):
        view = self.view(slot, half, cols)
        self.send(view, view, s.at[slot, half], r.at[slot, half], self.p.twin)

    def to_pair(self, slot, half):
        if self.p.paired:
            view = self.view(slot, half, pl.ds(self.give_o, self.pair_w))
            self.send(view, view, self.pair_s.at[slot, half], self.pair_r.at[slot, half], self.p.pair)

    def own(self, half):
        cols = self.ring_cols()
        src = self.view(0, half, cols)
        self.send(src, self.view(1, half, cols), self.ring_s.at[0, half], self.ring_r.at[1, half], self.p.along(1))
        self.send(
            src, self.view(2, half, cols), self.ring_s.at[self.opposite, half], self.ring_r.at[2, half], self.p.along(-1)
        )
        self.to_twin(0, half, pl.ds(0, self.width), self.twin_s, self.twin_r)

    def got(self, slot, half):
        view = self.view(slot, half, self.ring_cols())
        remote(view, view, self.ring_s.at[slot, half], self.ring_r.at[slot, half], self.p.along(1)).wait_recv()

    def tick(self, step, half):
        cols = self.ring_cols()
        if step == self.last:
            slots = (self.opposite,)
            self.got(self.opposite, half)
        else:
            behind, ahead = slots = (2 * step - 1, 2 * step)
            if step + 1 < self.last:
                for slot, way in ((behind, 1), (ahead, -1)):
                    self.got(slot, half)
                    self.send(
                        self.view(slot, half, cols),
                        self.view(slot + 2, half, cols),
                        self.ring_s.at[slot, half],
                        self.ring_r.at[slot + 2, half],
                        self.p.along(way),
                    )
            else:
                self.got(behind, half)
                self.got(ahead, half)
                slot = behind + self.p.core
                self.send(
                    self.view(slot, half, cols),
                    self.view(self.opposite, half, cols),
                    self.ring_s.at[slot, half],
                    self.ring_r.at[self.opposite, half],
                    self.p.along(1 - 2 * self.p.core),
                )
        for slot in slots:
            self.to_pair(slot, half)
            self.to_twin(slot, half, cols, self.twin_s, self.twin_r)

    def pair_tick(self, step, half):
        slots = (self.opposite,) if step == self.last else (2 * step - 1, 2 * step)
        if half == self.halves - 1:
            self.handed.update(slots)
        if not self.p.paired:
            return
        cols = pl.ds(self.pair_o, self.pair_w)
        for slot in slots:
            view = self.view(slot, half, cols)
            remote(view, view, self.pair_s.at[slot, half], self.pair_r.at[slot, half], self.p.pair).wait_recv()
            self.to_twin(slot, half, cols, self.twin2_s, self.twin2_r)

    def ready(self, slot):
        for half in range(self.halves):
            cols = pl.ds(0, self.width) if slot == 0 else self.ring_cols()
            view = self.view(slot, half, cols, 1 - self.p.core)
            remote(view, view, self.twin_s.at[slot, half], self.twin_r.at[slot, half], self.p.twin).wait_recv()
            if self.p.paired and slot > 0:
                view = self.view(slot, half, pl.ds(self.pair_o, self.pair_w), 1 - self.p.core)
                remote(view, view, self.twin2_s.at[slot, half], self.twin2_r.at[slot, half], self.p.twin).wait_recv()

    def drain(self):
        for copy in self.started:
            copy.wait_send()


def order(gate_up, down, last):
    late = []

    def one(stream, step, half):
        while len(late) > PAIR_LAG:
            a, b, c = late.pop(0)
            a.pair_tick(b, c)
        stream.tick(step, half)
        late.append((stream, step, half))

    for step in range(1, last + DOWN_LAG + 1):
        for half in range(gate_up.halves):
            if step <= last:
                one(gate_up, step, half)
                yield
        for half in range(down.halves):
            if step == DOWN_LAG:
                down.own(half)
            elif step > DOWN_LAG:
                one(down, step - DOWN_LAG, half)
                yield
    for a, b, c in late:
        a.pair_tick(b, c)


def all_to_all(place, src, dst, send_sem, recv_sem):
    chips = place.chips

    def body(t, _):
        step = chips // 2 + (1 - 2 * lax.rem(t, 2)) * lax.div(t + 1, 2)
        to = lax.rem(place.z + step, chips)
        for s, d, ss, rs in zip(src(to), dst(place.z), send_sem, recv_sem):
            remote(s, d, ss, rs, {"sp": 2 * to + place.core}).start()
        return 0

    lax.fori_loop(0, chips - 1, body, 0)


def wait_bytes(view, sem):
    pltpu.make_async_copy(view, view, sem).wait()


def layer(
    groups, spans, peers,
    q_hbm, k_hbm, v_hbm, g_hbm, ld_hbm, hg_hbm, wo_hbm, res_hbm, ng_hbm, gw_hbm, uw_hbm, dw_hbm, gt_hbm, ut_hbm,
    out_ref,
    q_ref, k_ref, v_ref, g_ref, ld_ref, hg_ref, ng_ref, gt_ref, ut_ref, gu, dn, wo, res, st, st_twin, dec, dec_twin, st_send, st_recv, dec_send, dec_recv, in_send, in_recv, in_twin, inner, grow, mix, att, att_r,
    mid, nsend, nall, nperm, pre, halo_s, halo_r, hid, ff, ff_r,
    load_sem, twin_s, twin_r, a2a_s, a2a_r, rs1_s, rs1_r, ag_s, ag_r, halo_ss, halo_rs, rs2_s, rs2_r,
    g0, g1, g2, g3, g4, g5, g6, g7, d0, d1, d2, d3, d4, d5, d6, d7,
):
    place = Place(groups, spans, peers)
    sp, tp, core = place.sp, place.tp, place.core
    length = q_hbm.shape[0]
    heads = q_hbm.shape[1] // HEAD
    combos = 2 * heads
    share = length // peers
    half_w = gw_hbm.shape[1]
    block = gw_hbm.shape[0]
    slots = place.chips
    scale = HEAD ** (-0.5)

    own_rows = pl.ds(pl.multiple_of(core * block, block), block)
    pairs = [
        (q_hbm, q_ref), (k_hbm, k_ref), (v_hbm, v_ref), (ld_hbm, ld_ref),
        (gw_hbm, gu.at[own_rows, pl.ds(0, half_w)]), (uw_hbm, gu.at[own_rows, pl.ds(half_w, half_w)]),
        (dw_hbm, dn.at[own_rows, :]), (g_hbm, g_ref), (hg_hbm, hg_ref), (wo_hbm, wo),
        (res_hbm.at[pl.ds(pl.multiple_of(tp * share, share), share), :], res), (ng_hbm, ng_ref), (gt_hbm, gt_ref),
        (ut_hbm, ut_ref),
    ]
    loads = [pltpu.make_async_copy(src, dst, load_sem.at[n]) for n, (src, dst) in enumerate(pairs)]
    for copy in loads:
        copy.start()

    barrier = pltpu.get_barrier_semaphore()

    def greet(step, _):
        pl.semaphore_signal(barrier, inc=1, device_id=place.along(step), device_id_type=MESH)
        return 0

    lax.fori_loop(1, place.chips, greet, 0)
    beside = {"sp": place.span(2 * core - 1)}
    for device in [place.twin, beside] + [{"tp": place.peer(step)} for step in range(1, peers)]:
        pl.semaphore_signal(barrier, inc=1, device_id=device, device_id_type=MESH)
    greeted = place.chips + peers
    if place.paired:
        pl.semaphore_signal(barrier, inc=1, device_id=place.pair, device_id_type=MESH)
        greeted += 1

    for copy in loads[:4]:
        copy.wait()
    row = lax.broadcasted_iota(jnp.int32, (HEAD, LANE), 0)
    lane = lax.broadcasted_iota(jnp.int32, (HEAD, LANE), 1)
    rates = [ld_ref[d, pl.ds(h, 1), :] for h in range(heads) for d in range(2)]
    sums = jnp.concatenate(rates + rates[: (-combos) % 8], axis=0) if combos % 8 else jnp.concatenate(rates, axis=0)
    s_lane = lax.broadcasted_iota(jnp.int32, sums.shape, 1)
    s_row = lax.broadcasted_iota(jnp.int32, sums.shape, 0)
    back = (s_row & 1) == 1
    shift = 1
    while shift < length:
        fwd = jnp.where(s_lane >= shift, pltpu.roll(sums, shift, 1), 0.0)
        bwd = jnp.where(s_lane < length - shift, pltpu.roll(sums, length - shift, 1), 0.0)
        sums = sums + jnp.where(back, bwd, fwd)
        shift *= 2
    chips = place.chips
    part = chips // 2
    rows = HEAD // part
    for h in range(heads):
        cols = pl.ds(h * HEAD, HEAD)
        q, k, v = q_ref[:, cols], k_ref[:, cols], v_ref[:, cols]
        v32 = v.astype(F32)
        scores = nt(q, k) * scale
        for d in range(2):
            m = 2 * h + d
            along_s = jnp.broadcast_to(sums[m : m + 1, :], (length, LANE))
            along_t = along_s.T
            seen = (row >= lane) if d == 0 else (row <= lane)
            decay = jnp.where(seen, jnp.exp(jnp.minimum(along_t - along_s, 0.0)), 0.0)
            inner[m] = nn((scores * decay).astype(BF16), v)
            grow[m] = jnp.exp(along_t) * scale
            total = along_t[length - 1 : length, :] if d == 0 else along_t[0:1, :]
            dec[m] = jnp.exp(total)
            faded = (v32 * jnp.exp(jnp.minimum(total - along_t, 0.0))).astype(BF16)
            st[m] = tn(k, faded).astype(BF16)

    gate_up = Stream(place, gu, GU_PARTS, (g0, g1, g2, g3, g4, g5, g6, g7))
    down = Stream(place, dn, DOWN_PARTS, (d0, d1, d2, d3, d4, d5, d6, d7))
    ring = order(gate_up, down, place.chips // 2)

    def advance(n):
        for _ in range(n):
            next(ring, None)

    def ready(stream, first, end):
        for slot in range(first, end):
            while slot not in stream.handed:
                next(ring, None)
            stream.ready(slot)

    for copy in loads[4:7]:
        copy.wait()
    pl.semaphore_wait(barrier, greeted)

    swaps = [
        remote(st, st_twin, twin_s.at[0], twin_r.at[0], place.twin),
        remote(dec, dec_twin, twin_s.at[1], twin_r.at[1], place.twin),
    ]
    for copy in swaps:
        copy.start()
    for part_no in range(OWN_FIRST):
        gate_up.own(part_no)
    for copy in swaps:
        copy.wait_recv()
    second = (core == 1).astype(F32)
    for d in range(2):
        m = 2 * core + d
        far = second if d == 0 else 1.0 - second
        mine, other = st[m].astype(F32), st_twin[m].astype(F32)
        my_dec, other_dec = dec[m], dec_twin[m]
        merged = mine * (far + (1.0 - far) * other_dec) + other * ((1.0 - far) + far * my_dec)
        st_send[pl.ds(d * part, part)] = merged.astype(BF16).reshape(part, rows, HEAD)
        dec_send[d] = my_dec * other_dec
    all_to_all(
        place,
        lambda to: (st_send.at[to], dec_send.at[lax.div(to, part)]),
        lambda me: (st_recv.at[me], dec_recv.at[me]),
        (a2a_s.at[0], a2a_s.at[1]),
        (a2a_r.at[0], a2a_r.at[1]),
    )
    for part_no in range(OWN_FIRST, GU_PARTS):
        gate_up.own(part_no)
    reverse = lax.div(place.z, part)
    st_recv[pl.ds(place.z, 1)] = st_send[pl.ds(place.z, 1)]
    dec_recv[pl.ds(place.z, 1)] = dec_send[pl.ds(reverse, 1)]
    advance(ADVANCE[0])
    others = pl.ds(0, chips - 1)
    wait_bytes(st_recv.at[others], a2a_r.at[0])
    wait_bytes(dec_recv.at[others], a2a_r.at[1])

    def scan(j, carry):
        at = j + reverse * (chips - 1 - 2 * j)
        in_send[at] = carry.astype(BF16)
        return carry * dec_recv[at] + st_recv[at].astype(F32)

    lax.fori_loop(0, chips, scan, jnp.zeros((rows, HEAD), F32))
    all_to_all(
        place, lambda to: (in_send.at[to],), lambda me: (in_recv.at[core, me],), (a2a_s.at[2],), (a2a_r.at[2],)
    )
    in_recv[core, pl.ds(place.z, 1)] = in_send[pl.ds(place.z, 1)]
    advance(ADVANCE[1])
    wait_bytes(in_recv.at[core, others], a2a_r.at[2])
    handover = remote(in_recv.at[core], in_twin, twin_s.at[2], twin_r.at[2], place.twin)
    handover.start()
    for copy in loads[7:]:
        copy.wait()
    handover.wait_recv()
    in_recv[1 - core] = in_twin[...]

    def normed_head(x):
        centre = x - jnp.mean(x, axis=1, keepdims=True)
        spread = jnp.mean(centre * centre, axis=1, keepdims=True)
        return centre * lax.rsqrt(spread + GROUP_EPS)

    for h in range(heads):
        cols = pl.ds(h * HEAD, HEAD)
        q = q_ref[:, cols]
        combined = None
        for d in range(2):
            m = 2 * h + d
            state = in_recv[h, pl.ds(d * part, part)].reshape(HEAD, HEAD).astype(F32)
            far = second if d == 0 else 1.0 - second
            state = state * (far * dec_twin[m] + (1.0 - far)) + far * st_twin[m].astype(F32)
            state = state.astype(BF16)
            term = normed_head(inner[m] + grow[m] * nn(q, state)) * hg_ref[pl.ds(d, 1), cols]
            combined = term if combined is None else combined + term
        gate = g_ref[:, cols].astype(F32)
        mix[:, cols] = (gate / (1.0 + jnp.exp(-gate)) * combined).astype(BF16)

    width = wo.shape[1]
    tile = min(512, width)
    for n in range(width // tile):
        cols = pl.ds(n * tile, tile)
        att[:, cols] = nn(mix[...], wo[:, cols]).astype(BF16)

    def peer_rows(j):
        return pl.ds(pl.multiple_of(j * share, share), share)

    started = []

    def to_peers(src, dst, s, r):
        for step in range(1, peers):
            copy = remote(src(place.peer(step)), dst(step), s.at[step - 1], r.at[step - 1], {"tp": place.peer(step)})
            copy.start()
            started.append(copy)

    to_peers(lambda j: att.at[peer_rows(j), :], lambda step: att_r.at[step - 1], rs1_s, rs1_r)
    advance(ADVANCE[2])
    for step in range(1, peers):
        remote(att_r.at[step - 1], att_r.at[step - 1], rs1_s.at[step - 1], rs1_r.at[step - 1], {"tp": tp}).wait_recv()
    total = att[peer_rows(tp), :].astype(F32)
    for step in range(1, peers):
        total = total + att_r[step - 1].astype(F32)
    middle = (res[...].astype(F32) + total).astype(BF16)
    mid[...] = middle
    values = middle.astype(F32)
    multiplier = lax.rsqrt(jnp.mean(values * values, axis=1, keepdims=True) + NORM_EPS)
    normed = (values * multiplier * ng_ref[...].astype(F32).reshape(1, -1)).astype(BF16)
    nsend[...] = normed
    nall[peer_rows(tp), :] = normed
    to_peers(lambda j: nsend, lambda step: nall.at[peer_rows(tp), :], ag_s, ag_r)
    advance(ADVANCE[3])
    for step in range(1, peers):
        view = nall.at[peer_rows(place.peer(peers - step)), :]
        remote(view, view, ag_s.at[step - 1], ag_r.at[step - 1], {"tp": tp}).wait_recv()
    for slot in range(slots):
        start = pl.multiple_of(place.slot_chip(slot) * LANE, LANE)
        nperm[:, pl.ds(slot * LANE, LANE)] = nall[:, pl.ds(start, LANE)]

    advance(ADVANCE[4])
    early = slots - 3
    ready(gate_up, 0, early)
    n_tile = 256 if (2 * half_w) % 256 == 0 else 128
    head_k, tail_k = pl.ds(0, early * 2 * block), pl.ds(early * 2 * block, (slots - early) * 2 * block)

    def tile_cols(n):
        return pl.ds(pl.multiple_of(n * n_tile, n_tile), n_tile)

    def project(n, _):
        pre[:, tile_cols(n)] = nn(nperm[:, head_k], gu[head_k, tile_cols(n)])
        return 0

    lax.fori_loop(0, 2 * half_w // n_tile, project, 0)
    ready(gate_up, early, slots)

    def project_rest(n, _):
        total = pre[:, tile_cols(n)] + nn(nperm[:, tail_k], gu[tail_k, tile_cols(n)])
        pre[:, tile_cols(n)] = total.astype(BF16).astype(F32)
        return 0

    lax.fori_loop(0, 2 * half_w // n_tile, project_rest, 0)
    halo_s[0] = pre[0:1, :]
    halo_s[1] = pre[length - 1 : length, :]
    before, after = {"sp": place.span(-1)}, {"sp": place.span(1)}
    halos = [
        remote(halo_s.at[0], halo_r.at[1], halo_ss.at[0], halo_rs.at[1], before),
        remote(halo_s.at[1], halo_r.at[0], halo_ss.at[1], halo_rs.at[0], after),
    ]
    for copy in halos:
        copy.start()
    advance(ADVANCE[5])
    for copy in halos:
        copy.wait_recv()
    not_first = (sp > 0).astype(F32)
    not_last = (sp < spans - 1).astype(F32)

    def conv(n, _):
        results = []
        for base, taps in ((0, gt_ref), (half_w, ut_ref)):
            cols = pl.ds(pl.multiple_of(base + n * LANE, LANE), LANE)
            x = pre[:, cols]
            above = jnp.where(row == 0, halo_r[0, :, cols] * not_first, pltpu.roll(x, 1, 0))
            below = jnp.where(row == length - 1, halo_r[1, :, cols] * not_last, pltpu.roll(x, length - 1, 0))
            t = taps[:, pl.ds(pl.multiple_of(n * LANE, LANE), LANE)].astype(F32)
            results.append(t[0:1] * above + t[1:2] * x + t[2:3] * below)
        gate, up = results
        hid[:, pl.ds(pl.multiple_of(n * LANE, LANE), LANE)] = (gate / (1.0 + jnp.exp(-gate)) * up).astype(BF16)
        return 0

    lax.fori_loop(0, half_w // LANE, conv, 0)

    cuts = sorted({0, slots // 2, slots - 2, slots})
    pieces = list(zip(cuts[:-1], cuts[1:]))
    for part_no, (lo, hi) in enumerate(pieces):
        ready(down, lo, hi)

        def project_down(n, _):
            rows_ = pl.ds(pl.multiple_of(n * 2 * LANE, 2 * LANE), 2 * LANE)
            ff[:, rows_] = nt(hid[...], dn[rows_, :]).astype(BF16)
            return 0

        lax.fori_loop(lo // 2, hi // 2, project_down, 0)
        cols = pl.ds(lo * LANE, (hi - lo) * LANE)
        to_peers(
            lambda j: ff.at[peer_rows(j), cols],
            lambda step: ff_r.at[step - 1, :, cols],
            rs2_s.at[part_no],
            rs2_r.at[part_no],
        )
    for part_no, (lo, hi) in enumerate(pieces):
        cols = pl.ds(lo * LANE, (hi - lo) * LANE)
        for step in range(1, peers):
            view = ff_r.at[step - 1, :, cols]
            remote(view, view, rs2_s.at[part_no, step - 1], rs2_r.at[part_no, step - 1], {"tp": tp}).wait_recv()
        for slot in range(lo, hi):
            held = pl.ds(slot * LANE, LANE)
            home = pl.ds(pl.multiple_of(place.slot_chip(slot) * LANE, LANE), LANE)
            total = ff[peer_rows(tp), held].astype(F32)
            for step in range(1, peers):
                total = total + ff_r[step - 1, :, held].astype(F32)
            out_ref[:, home] = (mid[:, home].astype(F32) + total).astype(BF16)

    advance(10_000)
    for copy in started + halos:
        copy.wait_send()
    for copy in swaps + [handover]:
        copy.wait_send()
    wait_bytes(st_send.at[others], a2a_s.at[0])
    wait_bytes(dec_recv.at[others], a2a_s.at[1])
    wait_bytes(in_send.at[others], a2a_s.at[2])
    gate_up.drain()
    down.drain()


PAIRED = True
OWN_FIRST = 1
RING_SHARE = 0.66
PAIR_LAG = 2
DOWN_LAG = 1
GU_PARTS = 2
DOWN_PARTS = 2
ADVANCE = (4, 7, 4, 4, 0, 2)


def solution(mesh):
    groups, spans, peers = mesh.shape["grp"], mesh.shape["sp"], mesh.shape["tp"]
    rows_, cols_ = ("grp", "sp"), "tp"
    placed = (
        P(rows_, cols_), P(rows_, cols_), P(rows_, cols_), P(rows_, cols_), P(None, cols_, rows_), P(None, cols_),
        P(cols_, None), P(rows_, None), P(), P("sp", cols_), P("sp", cols_), P("sp", cols_), P(None, cols_),
        P(None, cols_),
    )

    def shards(q, k, v, g, ld, hg, wo, res, ng, gw, uw, dw, gt, ut):
        length = q.shape[0]
        heads = q.shape[1] // HEAD
        combos = 2 * heads
        share = length // peers
        block, half_w = gw.shape
        width = wo.shape[1]
        chips = spans // 2
        packet = 2 * HEAD // chips
        dma = pltpu.SemaphoreType.DMA
        vmem = pl.BlockSpec(memory_space=pltpu.VMEM)
        hbm = pl.BlockSpec(memory_space=pltpu.HBM)
        scratch = [pltpu.VMEM(a.shape, a.dtype) for a in (q, k, v, g, ld, hg, ng, gt, ut)] + [
            pltpu.VMEM((spans * block, 2 * half_w), BF16),
            pltpu.VMEM((spans * block, half_w), BF16),
            pltpu.VMEM(wo.shape, BF16),
            pltpu.VMEM((share, width), BF16),
            pltpu.VMEM((combos, HEAD, HEAD), BF16),
            pltpu.VMEM((combos, HEAD, HEAD), BF16),
            pltpu.VMEM((combos, 1, LANE), F32),
            pltpu.VMEM((combos, 1, LANE), F32),
            pltpu.VMEM((chips, packet, HEAD), BF16),
            pltpu.VMEM((chips, packet, HEAD), BF16),
            pltpu.VMEM((2, 1, LANE), F32),
            pltpu.VMEM((chips, 1, LANE), F32),
            pltpu.VMEM((chips, packet, HEAD), BF16),
            pltpu.VMEM((2, chips, packet, HEAD), BF16),
            pltpu.VMEM((chips, packet, HEAD), BF16),
            pltpu.VMEM((combos, length, HEAD), F32),
            pltpu.VMEM((combos, length, HEAD), F32),
            pltpu.VMEM((length, heads * HEAD), BF16),
            pltpu.VMEM((length, width), BF16),
            pltpu.VMEM((peers - 1, share, width), BF16),
            pltpu.VMEM((share, width), BF16),
            pltpu.VMEM((share, width), BF16),
            pltpu.VMEM((length, width), BF16),
            pltpu.VMEM((length, width), BF16),
            pltpu.VMEM((length, 2 * half_w), F32),
            pltpu.VMEM((2, 1, 2 * half_w), F32),
            pltpu.VMEM((2, 1, 2 * half_w), F32),
            pltpu.VMEM((length, half_w), BF16),
            pltpu.VMEM((length, width), BF16),
            pltpu.VMEM((peers - 1, share, width), BF16),
            dma((14,)), dma((3,)), dma((3,)), dma((3,)), dma((3,)), dma((peers - 1,)), dma((peers - 1,)), dma((peers - 1,)), dma((peers - 1,)),
            dma((2,)), dma((2,)), dma((3, peers - 1)), dma((3, peers - 1)),
        ] + [dma((chips, n)) for n in (GU_PARTS, DOWN_PARTS) for _ in range(8)]
        return pl.pallas_call(
            functools.partial(layer, groups, spans, peers),
            name="layer",
            out_shape=jax.ShapeDtypeStruct((share, width), BF16),
            in_specs=[hbm] * 14,
            out_specs=vmem,
            scratch_shapes=scratch,
            compiler_params=pltpu.CompilerParams(
                collective_id=0, has_side_effects=True, vmem_limit_bytes=67_043_328
            ),
        )(q, k, v, g, ld, hg, wo, res, ng, gw, uw, dw, gt, ut)

    return jax.shard_map(shards, mesh=mesh, in_specs=placed, out_specs=P(("grp", "sp", "tp"), None), check_vma=False)
```

```python
import functools

import jax
import jax.numpy as jnp
from jax import lax
from jax.experimental import pallas as pl
from jax.experimental.pallas import tpu as pltpu
from jax.sharding import PartitionSpec as P

HEAD = 128
LANE = 128
GROUP_EPS = 1e-05
NORM_EPS = 1e-06
MESH = pl.DeviceIdType.MESH
F32 = jnp.float32
BF16 = jnp.bfloat16


def nt(a, b):
    return lax.dot_general(a, b, (((1,), (1,)), ((), ())), preferred_element_type=F32)


def tn(a, b):
    return lax.dot_general(a, b, (((0,), (0,)), ((), ())), preferred_element_type=F32)


def nn(a, b):
    return jnp.dot(a, b, preferred_element_type=F32)


def groups_of(slots):
    early = slots - EARLY
    cuts = sorted({0, slots // 2, slots - 2, slots})
    return [(0, early), (early, slots)], list(zip(cuts[:-1], cuts[1:]))


class Place:
    def __init__(self, groups, spans, peers):
        self.spans, self.peers, self.chips = spans, peers, spans // 2
        self.sp = lax.axis_index("sp")
        self.tp = lax.axis_index("tp")
        self.core = lax.rem(self.sp, 2)
        self.z = lax.div(self.sp, 2)
        self.paired = PAIRED and groups % 2 == 0
        grp = lax.axis_index("grp")
        self.side = lax.rem(grp, 2)
        self.pair = {"grp": grp + 1 - 2 * self.side}
        self.twin = {"sp": self.sp + 1 - 2 * self.core}

    def chip(self, step):
        return lax.rem(self.z + step + self.chips, self.chips)

    def along(self, step):
        return {"sp": 2 * self.chip(step) + self.core}

    def span(self, step):
        return lax.rem(self.sp + step + self.spans, self.spans)

    def peer(self, step):
        return lax.rem(self.tp + step, self.peers)

    def slot_chip(self, slot):
        step = (slot + 1) // 2
        return self.chip(-step if slot % 2 else step)


def remote(src, dst, send_sem, recv_sem, device):
    return pltpu.make_async_remote_copy(
        src_ref=src, dst_ref=dst, send_sem=send_sem, recv_sem=recv_sem, device_id=device, device_id_type=MESH
    )


class Stream:
    def __init__(self, place, buf, share, parts, groups, send_s, ring_r, pair_r, twin_r):
        self.p, self.buf, self.parts, self.groups = place, buf, parts, groups
        self.ring_s, self.pair_s, self.twin_s = (send_s.at[n] for n in range(3))
        self.ring_r, self.pair_r, self.twin_r = ring_r, pair_r, twin_r
        width = buf.shape[1]
        tiles = width // LANE
        ring = max((tiles + 1) // 2, int(share * tiles)) if place.paired else tiles
        self.width = width
        self.ring_w = ring * LANE
        self.pair_w = width - self.ring_w
        self.ring_o = pl.multiple_of(place.side * self.pair_w, LANE) if place.paired else 0
        self.pair_o = pl.multiple_of((1 - place.side) * self.ring_w, LANE)
        self.give_o = pl.multiple_of(place.side * self.ring_w, LANE)
        self.block = buf.shape[0] // place.spans
        self.rows = self.block // parts
        self.last = place.chips // 2
        self.opposite = place.chips - 1
        self.handed = {0}

    def view(self, slot, part, cols):
        start = pl.multiple_of(slot * 2 * self.block + self.p.core * self.block + part * self.rows, self.rows)
        return self.buf.at[pl.ds(start, self.rows), cols]

    def bulk(self, rows, width):
        return self.buf.at[pl.ds(0, rows), pl.ds(0, width)]

    def ring_cols(self):
        return pl.ds(self.ring_o, self.ring_w)

    def slots(self, step):
        return (self.opposite,) if step == self.last else (2 * step - 1, 2 * step)

    def on(self, src_slot, dst_slot, part, way):
        cols = self.ring_cols()
        src, dst = self.view(src_slot, part, cols), self.view(dst_slot, part, cols)
        remote(src, dst, self.ring_s, self.ring_r.at[dst_slot, part], self.p.along(way)).start()

    def to_twin(self, slot, part, cols):
        view = self.view(slot, part, cols)
        group = [n for n, (lo, hi) in enumerate(self.groups) if lo <= slot < hi][0]
        remote(view, view, self.twin_s, self.twin_r.at[group], self.p.twin).start()

    def own(self, part):
        self.on(0, 1, part, 1)
        self.on(0, 2, part, -1)
        self.to_twin(0, part, pl.ds(0, self.width))

    def got(self, slot, part):
        view = self.view(slot, part, self.ring_cols())
        wait_bytes(view, self.ring_r.at[slot, part])

    def tick(self, step, part):
        if step == self.last:
            self.got(self.opposite, part)
        else:
            behind, ahead = self.slots(step)
            if step + 1 < self.last:
                self.got(behind, part)
                self.on(behind, behind + 2, part, 1)
                self.got(ahead, part)
                self.on(ahead, ahead + 2, part, -1)
            else:
                self.got(behind, part)
                self.got(ahead, part)
                self.on(behind + self.p.core, self.opposite, part, 1 - 2 * self.p.core)
        for slot in self.slots(step):
            if self.p.paired:
                view = self.view(slot, part, pl.ds(self.give_o, self.pair_w))
                remote(view, view, self.pair_s, self.pair_r.at[step, part], self.p.pair).start()
        for slot in self.slots(step):
            self.to_twin(slot, part, self.ring_cols())

    def pair_tick(self, step, part):
        slots = self.slots(step)
        if part == self.parts - 1:
            self.handed.update(slots)
        if not self.p.paired:
            return
        wait_bytes(self.bulk(len(slots) * self.rows, self.pair_w), self.pair_r.at[step, part])
        for slot in slots:
            self.to_twin(slot, part, pl.ds(self.pair_o, self.pair_w))

    def ready(self, group):
        lo, hi = self.groups[group]
        wait_bytes(self.bulk((hi - lo) * self.block, self.width), self.twin_r.at[group])

    def drain(self):
        rest = (self.p.chips - 1) * self.block
        wait_bytes(self.bulk(rest, self.ring_w), self.ring_s)
        if self.p.paired:
            wait_bytes(self.bulk(rest, self.pair_w), self.pair_s)
        wait_bytes(self.bulk(rest + self.block, self.width), self.twin_s)


def order(gate_up, down, last):
    late = []

    def one(stream, step, part):
        while len(late) > PAIR_LAG:
            a, b, c = late.pop(0)
            a.pair_tick(b, c)
        stream.tick(step, part)
        late.append((stream, step, part))

    for step in range(1, last + DOWN_LAG + 1):
        for part in range(gate_up.parts):
            if step <= last:
                one(gate_up, step, part)
                yield
        for part in range(down.parts):
            if step == DOWN_LAG:
                down.own(part)
            elif step > DOWN_LAG:
                one(down, step - DOWN_LAG, part)
                yield
    for a, b, c in late:
        a.pair_tick(b, c)


def all_to_all(place, src, dst, send_sem, recv_sem):
    chips = place.chips

    def body(t, _):
        step = chips // 2 + (1 - 2 * lax.rem(t, 2)) * lax.div(t + 1, 2)
        to = lax.rem(place.z + step, chips)
        for s, d, ss, rs in zip(src(to), dst(place.z), send_sem, recv_sem):
            remote(s, d, ss, rs, {"sp": 2 * to + place.core}).start()
        return 0

    lax.fori_loop(0, chips - 1, body, 0)


def wait_bytes(view, sem):
    pltpu.make_async_copy(view, view, sem).wait()


def layer(
    groups, spans, peers,
    q_hbm, k_hbm, v_hbm, g_hbm, ld_hbm, hg_hbm, wo_hbm, res_hbm, ng_hbm, gw_hbm, uw_hbm, dw_hbm, gt_hbm, ut_hbm,
    out_ref,
    q_ref, k_ref, v_ref, g_ref, ld_ref, hg_ref, ng_ref, gt_ref, ut_ref, gu, dn, wo, res, st, st_twin, dec, dec_twin, st_send, st_recv, dec_send, dec_recv, in_send, in_recv, in_twin, inner, grow, mix, att, att_r,
    mid, nsend, nall, nperm, pre, halo_s, halo_r, hid, ff, ff_r,
    load_sem, twin_s, twin_r, a2a_s, a2a_r, tp_s, tp_r, halo_ss, halo_rs,
    gu_s, gu_ring, gu_pair, gu_twin, dn_s, dn_ring, dn_pair, dn_twin,
):
    place = Place(groups, spans, peers)
    sp, tp, core = place.sp, place.tp, place.core
    length = q_hbm.shape[0]
    heads = q_hbm.shape[1] // HEAD
    combos = 2 * heads
    share = length // peers
    half_w = gw_hbm.shape[1]
    block = gw_hbm.shape[0]
    slots = place.chips
    scale = HEAD ** (-0.5)

    own_rows = pl.ds(pl.multiple_of(core * block, block), block)
    pairs = [
        (q_hbm, q_ref), (k_hbm, k_ref), (v_hbm, v_ref), (ld_hbm, ld_ref),
        (gw_hbm, gu.at[own_rows, pl.ds(0, half_w)]), (uw_hbm, gu.at[own_rows, pl.ds(half_w, half_w)]),
        (dw_hbm, dn.at[own_rows, :]), (g_hbm, g_ref), (hg_hbm, hg_ref), (wo_hbm, wo),
        (res_hbm.at[pl.ds(pl.multiple_of(tp * share, share), share), :], res), (ng_hbm, ng_ref), (gt_hbm, gt_ref),
        (ut_hbm, ut_ref),
    ]
    loads = [pltpu.make_async_copy(src, dst, load_sem.at[n]) for n, (src, dst) in enumerate(pairs)]
    for copy in loads:
        copy.start()

    barrier = pltpu.get_barrier_semaphore()

    def greet(step, _):
        pl.semaphore_signal(barrier, inc=1, device_id=place.along(step), device_id_type=MESH)
        return 0

    lax.fori_loop(1, place.chips, greet, 0)
    beside = {"sp": place.span(2 * core - 1)}
    for device in [place.twin, beside] + [{"tp": place.peer(step)} for step in range(1, peers)]:
        pl.semaphore_signal(barrier, inc=1, device_id=device, device_id_type=MESH)
    greeted = place.chips + peers
    if place.paired:
        pl.semaphore_signal(barrier, inc=1, device_id=place.pair, device_id_type=MESH)
        greeted += 1

    for copy in loads[:4]:
        copy.wait()
    row = lax.broadcasted_iota(jnp.int32, (HEAD, LANE), 0)
    lane = lax.broadcasted_iota(jnp.int32, (HEAD, LANE), 1)
    rates = [ld_ref[d, pl.ds(h, 1), :] for h in range(heads) for d in range(2)]
    sums = jnp.concatenate(rates + rates[: (-combos) % 8], axis=0) if combos % 8 else jnp.concatenate(rates, axis=0)
    s_lane = lax.broadcasted_iota(jnp.int32, sums.shape, 1)
    s_row = lax.broadcasted_iota(jnp.int32, sums.shape, 0)
    back = (s_row & 1) == 1
    shift = 1
    while shift < length:
        fwd = jnp.where(s_lane >= shift, pltpu.roll(sums, shift, 1), 0.0)
        bwd = jnp.where(s_lane < length - shift, pltpu.roll(sums, length - shift, 1), 0.0)
        sums = sums + jnp.where(back, bwd, fwd)
        shift *= 2
    chips = place.chips
    part = chips // 2
    rows = HEAD // part
    for h in range(heads):
        cols = pl.ds(h * HEAD, HEAD)
        q, k, v = q_ref[:, cols], k_ref[:, cols], v_ref[:, cols]
        v32 = v.astype(F32)
        scores = nt(q, k) * scale
        for d in range(2):
            m = 2 * h + d
            along_s = jnp.broadcast_to(sums[m : m + 1, :], (length, LANE))
            along_t = along_s.T
            seen = (row >= lane) if d == 0 else (row <= lane)
            decay = jnp.where(seen, jnp.exp(jnp.minimum(along_t - along_s, 0.0)), 0.0)
            inner[m] = nn((scores * decay).astype(BF16), v)
            grow[m] = jnp.exp(along_t) * scale
            total = along_t[length - 1 : length, :] if d == 0 else along_t[0:1, :]
            dec[m] = jnp.exp(total)
            faded = (v32 * jnp.exp(jnp.minimum(total - along_t, 0.0))).astype(BF16)
            st[m] = tn(k, faded).astype(BF16)

    early, cuts = groups_of(slots)
    gate_up = Stream(place, gu, GU_SHARE, GU_PARTS, early, gu_s, gu_ring, gu_pair, gu_twin)
    down = Stream(place, dn, DOWN_SHARE, DOWN_PARTS, cuts, dn_s, dn_ring, dn_pair, dn_twin)
    ring = order(gate_up, down, place.chips // 2)

    def advance(n):
        for _ in range(n):
            next(ring, None)

    def ready(stream, group):
        while not stream.handed.issuperset(range(*stream.groups[group])):
            next(ring, None)
        stream.ready(group)

    for copy in loads[4:7]:
        copy.wait()
    pl.semaphore_wait(barrier, greeted)

    swaps = [
        remote(st, st_twin, twin_s.at[0], twin_r.at[0], place.twin),
        remote(dec, dec_twin, twin_s.at[1], twin_r.at[1], place.twin),
    ]
    for copy in swaps:
        copy.start()
    for part_no in range(OWN_FIRST):
        gate_up.own(part_no)
    for copy in swaps:
        copy.wait_recv()
    second = (core == 1).astype(F32)
    for d in range(2):
        m = 2 * core + d
        far = second if d == 0 else 1.0 - second
        mine, other = st[m].astype(F32), st_twin[m].astype(F32)
        my_dec, other_dec = dec[m], dec_twin[m]
        merged = mine * (far + (1.0 - far) * other_dec) + other * ((1.0 - far) + far * my_dec)
        st_send[pl.ds(d * part, part)] = merged.astype(BF16).reshape(part, rows, HEAD)
        dec_send[d] = my_dec * other_dec
    all_to_all(
        place,
        lambda to: (st_send.at[to], dec_send.at[lax.div(to, part)]),
        lambda me: (st_recv.at[me], dec_recv.at[me]),
        (a2a_s.at[0], a2a_s.at[1]),
        (a2a_r.at[0], a2a_r.at[1]),
    )
    for part_no in range(OWN_FIRST, GU_PARTS):
        gate_up.own(part_no)
    reverse = lax.div(place.z, part)
    st_recv[pl.ds(place.z, 1)] = st_send[pl.ds(place.z, 1)]
    dec_recv[pl.ds(place.z, 1)] = dec_send[pl.ds(reverse, 1)]
    advance(ADVANCE[0])
    others = pl.ds(0, chips - 1)
    wait_bytes(st_recv.at[others], a2a_r.at[0])
    wait_bytes(dec_recv.at[others], a2a_r.at[1])

    def scan(j, carry):
        at = j + reverse * (chips - 1 - 2 * j)
        in_send[at] = carry.astype(BF16)
        return carry * dec_recv[at] + st_recv[at].astype(F32)

    lax.fori_loop(0, chips, scan, jnp.zeros((rows, HEAD), F32))
    all_to_all(
        place, lambda to: (in_send.at[to],), lambda me: (in_recv.at[core, me],), (a2a_s.at[2],), (a2a_r.at[2],)
    )
    in_recv[core, pl.ds(place.z, 1)] = in_send[pl.ds(place.z, 1)]
    advance(ADVANCE[1])
    wait_bytes(in_recv.at[core, others], a2a_r.at[2])
    handover = remote(in_recv.at[core], in_twin, twin_s.at[2], twin_r.at[2], place.twin)
    handover.start()
    for copy in loads[7:]:
        copy.wait()
    advance(ADVANCE[2])
    handover.wait_recv()
    in_recv[1 - core] = in_twin[...]

    def normed_head(x):
        centre = x - jnp.mean(x, axis=1, keepdims=True)
        spread = jnp.mean(centre * centre, axis=1, keepdims=True)
        return centre * lax.rsqrt(spread + GROUP_EPS)

    for h in range(heads):
        cols = pl.ds(h * HEAD, HEAD)
        q = q_ref[:, cols]
        combined = None
        for d in range(2):
            m = 2 * h + d
            state = in_recv[h, pl.ds(d * part, part)].reshape(HEAD, HEAD).astype(F32)
            far = second if d == 0 else 1.0 - second
            state = state * (far * dec_twin[m] + (1.0 - far)) + far * st_twin[m].astype(F32)
            state = state.astype(BF16)
            term = normed_head(inner[m] + grow[m] * nn(q, state)) * hg_ref[pl.ds(d, 1), cols]
            combined = term if combined is None else combined + term
        gate = g_ref[:, cols].astype(F32)
        mix[:, cols] = (gate / (1.0 + jnp.exp(-gate)) * combined).astype(BF16)

    width = wo.shape[1]
    tile = min(512, width)
    for n in range(width // tile):
        cols = pl.ds(n * tile, tile)
        att[:, cols] = nn(mix[...], wo[:, cols]).astype(BF16)

    def peer_rows(j):
        return pl.ds(pl.multiple_of(j * share, share), share)

    def to_peers(src, dst, s, r):
        for step in range(1, peers):
            remote(src(place.peer(step)), dst(step), s, r, {"tp": place.peer(step)}).start()

    foreign = pl.ds(0, (peers - 1) * share)
    to_peers(lambda j: att.at[peer_rows(j), :], lambda step: att_r.at[step - 1], tp_s.at[0], tp_r.at[0])
    advance(ADVANCE[3])
    wait_bytes(att_r, tp_r.at[0])
    total = att[peer_rows(tp), :].astype(F32)
    for step in range(1, peers):
        total = total + att_r[step - 1].astype(F32)
    middle = (res[...].astype(F32) + total).astype(BF16)
    mid[...] = middle
    values = middle.astype(F32)
    multiplier = lax.rsqrt(jnp.mean(values * values, axis=1, keepdims=True) + NORM_EPS)
    normed = (values * multiplier * ng_ref[...].astype(F32).reshape(1, -1)).astype(BF16)
    nsend[...] = normed
    nall[peer_rows(tp), :] = normed
    to_peers(lambda j: nsend, lambda step: nall.at[peer_rows(tp), :], tp_s.at[1], tp_r.at[1])
    advance(ADVANCE[4])
    wait_bytes(nall.at[foreign, :], tp_r.at[1])
    halo_s[0] = nall[0:1, :].astype(F32)
    halo_s[1] = nall[length - 1 : length, :].astype(F32)
    before, after = {"sp": place.span(-1)}, {"sp": place.span(1)}
    halos = [
        remote(halo_s.at[0], halo_r.at[1], halo_ss.at[0], halo_rs.at[1], before),
        remote(halo_s.at[1], halo_r.at[0], halo_ss.at[1], halo_rs.at[0], after),
    ]
    for copy in halos:
        copy.start()
    for slot in range(slots):
        start = pl.multiple_of(place.slot_chip(slot) * LANE, LANE)
        nperm[0:length, pl.ds(slot * LANE, LANE)] = nall[:, pl.ds(start, LANE)]
    advance(ADVANCE[5])
    for copy in halos:
        copy.wait_recv()
    rim_row = lax.broadcasted_iota(jnp.int32, (RIM, LANE), 0)
    not_first = (sp > 0).astype(F32)
    not_last = (sp < spans - 1).astype(F32)
    for slot in range(slots):
        cols = pl.ds(pl.multiple_of(place.slot_chip(slot) * LANE, LANE), LANE)
        rim = jnp.where(rim_row == 0, halo_r[0, :, cols] * not_first, 0.0)
        rim = jnp.where(rim_row == 1, halo_r[1, :, cols] * not_last, rim)
        nperm[pl.ds(length, RIM), pl.ds(slot * LANE, LANE)] = rim.astype(BF16)

    ready(gate_up, 0)
    n_tile = 256 if (2 * half_w) % 256 == 0 else 128
    count = 2 * half_w // n_tile
    split_at = early[0][1] * 2 * block
    head_k, tail_k = pl.ds(0, split_at), pl.ds(split_at, spans * block - split_at)

    def tile_cols(n):
        return pl.ds(pl.multiple_of(n * n_tile, n_tile), n_tile)

    def project(n, _):
        pre[:, tile_cols(n)] = nn(nperm[:, head_k], gu[head_k, tile_cols(n)])
        return 0

    thirds = [count * n // 3 for n in range(4)]
    for lo, hi in zip(thirds[:-1], thirds[1:]):
        lax.fori_loop(lo, hi, project, 0)
        advance(ADVANCE[6])
    ready(gate_up, 1)

    def project_rest(n, _):
        total = pre[:, tile_cols(n)] + nn(nperm[:, tail_k], gu[tail_k, tile_cols(n)])
        pre[:, tile_cols(n)] = total.astype(BF16).astype(F32)
        return 0

    lax.fori_loop(0, count, project_rest, 0)
    advance(ADVANCE[7])
    def conv(n, _):
        results = []
        for base, taps in ((0, gt_ref), (half_w, ut_ref)):
            cols = pl.ds(pl.multiple_of(base + n * LANE, LANE), LANE)
            x = pre[0:length, cols]
            above = jnp.where(row == 0, pre[pl.ds(length, 1), cols], pltpu.roll(x, 1, 0))
            below = jnp.where(row == length - 1, pre[pl.ds(length + 1, 1), cols], pltpu.roll(x, length - 1, 0))
            t = taps[:, pl.ds(pl.multiple_of(n * LANE, LANE), LANE)].astype(F32)
            results.append(t[0:1] * above + t[1:2] * x + t[2:3] * below)
        gate, up = results
        hid[:, pl.ds(pl.multiple_of(n * LANE, LANE), LANE)] = (gate / (1.0 + jnp.exp(-gate)) * up).astype(BF16)
        return 0

    lax.fori_loop(0, half_w // LANE, conv, 0)

    for part_no, (lo, hi) in enumerate(cuts):
        ready(down, part_no)

        def project_down(n, _):
            rows_ = pl.ds(pl.multiple_of(n * 2 * LANE, 2 * LANE), 2 * LANE)
            ff[:, rows_] = nt(hid[...], dn[rows_, :]).astype(BF16)
            return 0

        lax.fori_loop(lo // 2, hi // 2, project_down, 0)
        cols = pl.ds(lo * LANE, (hi - lo) * LANE)
        to_peers(
            lambda j: ff.at[peer_rows(j), cols],
            lambda step: ff_r.at[step - 1, :, cols],
            tp_s.at[2 + part_no],
            tp_r.at[2 + part_no],
        )
    for part_no, (lo, hi) in enumerate(cuts):
        cols = pl.ds(lo * LANE, (hi - lo) * LANE)
        wait_bytes(ff_r.at[:, :, cols], tp_r.at[2 + part_no])
        for slot in range(lo, hi):
            held = pl.ds(slot * LANE, LANE)
            home = pl.ds(pl.multiple_of(place.slot_chip(slot) * LANE, LANE), LANE)
            total = ff[peer_rows(tp), held].astype(F32)
            for step in range(1, peers):
                total = total + ff_r[step - 1, :, held].astype(F32)
            out_ref[:, home] = (mid[:, home].astype(F32) + total).astype(BF16)

    advance(10_000)
    for copy in halos + swaps + [handover]:
        copy.wait_send()
    for n in range(2):
        wait_bytes(att_r, tp_s.at[n])
    for n, (lo, hi) in enumerate(cuts):
        wait_bytes(ff_r.at[:, :, pl.ds(lo * LANE, (hi - lo) * LANE)], tp_s.at[2 + n])
    wait_bytes(st_send.at[others], a2a_s.at[0])
    wait_bytes(dec_recv.at[others], a2a_s.at[1])
    wait_bytes(in_send.at[others], a2a_s.at[2])
    gate_up.drain()
    down.drain()


PAIRED = True
OWN_FIRST = 1
GU_SHARE = 0.69
DOWN_SHARE = 0.73
RIM = 16
EARLY = 1
PAIR_LAG = 2
DOWN_LAG = 2
GU_PARTS = 2
DOWN_PARTS = 2
ADVANCE = (4, 7, 1, 5, 5, 0, 1, 1)


def solution(mesh):
    groups, spans, peers = mesh.shape["grp"], mesh.shape["sp"], mesh.shape["tp"]
    rows_, cols_ = ("grp", "sp"), "tp"
    placed = (
        P(rows_, cols_), P(rows_, cols_), P(rows_, cols_), P(rows_, cols_), P(None, cols_, rows_), P(None, cols_),
        P(cols_, None), P(rows_, None), P(), P("sp", cols_), P("sp", cols_), P("sp", cols_), P(None, cols_),
        P(None, cols_),
    )

    def shards(q, k, v, g, ld, hg, wo, res, ng, gw, uw, dw, gt, ut):
        length = q.shape[0]
        heads = q.shape[1] // HEAD
        combos = 2 * heads
        share = length // peers
        block, half_w = gw.shape
        width = wo.shape[1]
        chips = spans // 2
        packet = 2 * HEAD // chips
        dma = pltpu.SemaphoreType.DMA
        vmem = pl.BlockSpec(memory_space=pltpu.VMEM)
        hbm = pl.BlockSpec(memory_space=pltpu.HBM)
        scratch = [pltpu.VMEM(a.shape, a.dtype) for a in (q, k, v, g, ld, hg, ng, gt, ut)] + [
            pltpu.VMEM((spans * block, 2 * half_w), BF16),
            pltpu.VMEM((spans * block, half_w), BF16),
            pltpu.VMEM(wo.shape, BF16),
            pltpu.VMEM((share, width), BF16),
            pltpu.VMEM((combos, HEAD, HEAD), BF16),
            pltpu.VMEM((combos, HEAD, HEAD), BF16),
            pltpu.VMEM((combos, 1, LANE), F32),
            pltpu.VMEM((combos, 1, LANE), F32),
            pltpu.VMEM((chips, packet, HEAD), BF16),
            pltpu.VMEM((chips, packet, HEAD), BF16),
            pltpu.VMEM((2, 1, LANE), F32),
            pltpu.VMEM((chips, 1, LANE), F32),
            pltpu.VMEM((chips, packet, HEAD), BF16),
            pltpu.VMEM((2, chips, packet, HEAD), BF16),
            pltpu.VMEM((chips, packet, HEAD), BF16),
            pltpu.VMEM((combos, length, HEAD), F32),
            pltpu.VMEM((combos, length, HEAD), F32),
            pltpu.VMEM((length, heads * HEAD), BF16),
            pltpu.VMEM((length, width), BF16),
            pltpu.VMEM((peers - 1, share, width), BF16),
            pltpu.VMEM((share, width), BF16),
            pltpu.VMEM((share, width), BF16),
            pltpu.VMEM((length, width), BF16),
            pltpu.VMEM((length + RIM, width), BF16),
            pltpu.VMEM((length + RIM, 2 * half_w), F32),
            pltpu.VMEM((2, 1, width), F32),
            pltpu.VMEM((2, 1, width), F32),
            pltpu.VMEM((length, half_w), BF16),
            pltpu.VMEM((length, width), BF16),
            pltpu.VMEM((peers - 1, share, width), BF16),
            dma((14,)), dma((3,)), dma((3,)), dma((3,)), dma((3,)), dma((5,)), dma((5,)), dma((2,)), dma((2,)),
        ]
        for parts, held in zip((GU_PARTS, DOWN_PARTS), groups_of(chips)):
            scratch += [dma((3,)), dma((chips, parts)), dma((chips // 2 + 1, parts)), dma((len(held),))]
        return pl.pallas_call(
            functools.partial(layer, groups, spans, peers),
            name="layer",
            out_shape=jax.ShapeDtypeStruct((share, width), BF16),
            in_specs=[hbm] * 14,
            out_specs=vmem,
            scratch_shapes=scratch,
            compiler_params=pltpu.CompilerParams(
                collective_id=0, has_side_effects=True, vmem_limit_bytes=67_043_328
            ),
        )(q, k, v, g, ld, hg, wo, res, ng, gw, uw, dw, gt, ut)

    return jax.shard_map(shards, mesh=mesh, in_specs=placed, out_specs=P(("grp", "sp", "tp"), None), check_vma=False)
```

```python
import functools

import jax
import jax.numpy as jnp
from jax import lax
from jax.experimental import pallas as pl
from jax.experimental.pallas import tpu as pltpu
from jax.sharding import PartitionSpec as P

HEAD = 128
LANE = 128
GROUP_EPS = 1e-05
NORM_EPS = 1e-06
MESH = pl.DeviceIdType.MESH
F32 = jnp.float32
BF16 = jnp.bfloat16


def nt(a, b):
    return lax.dot_general(a, b, (((1,), (1,)), ((), ())), preferred_element_type=F32)


def tn(a, b):
    return lax.dot_general(a, b, (((0,), (0,)), ((), ())), preferred_element_type=F32)


def nn(a, b):
    return jnp.dot(a, b, preferred_element_type=F32)


def groups_of(slots):
    early = slots - EARLY
    cuts = sorted({0, slots // 2, slots - 4, slots - 2, slots})
    return [(0, early), (early, slots)], list(zip(cuts[:-1], cuts[1:]))


class Place:
    def __init__(self, groups, spans, peers):
        self.spans, self.peers, self.chips = spans, peers, spans // 2
        self.sp = lax.axis_index("sp")
        self.tp = lax.axis_index("tp")
        self.core = lax.rem(self.sp, 2)
        self.z = lax.div(self.sp, 2)
        self.paired = PAIRED and groups % 2 == 0
        grp = lax.axis_index("grp")
        self.side = lax.rem(grp, 2)
        self.pair = {"grp": grp + 1 - 2 * self.side}
        self.twin = {"sp": self.sp + 1 - 2 * self.core}

    def chip(self, step):
        return lax.rem(self.z + step + self.chips, self.chips)

    def along(self, step):
        return {"sp": 2 * self.chip(step) + self.core}

    def span(self, step):
        return lax.rem(self.sp + step + self.spans, self.spans)

    def peer(self, step):
        return lax.rem(self.tp + step, self.peers)

    def slot_chip(self, slot):
        step = (slot + 1) // 2
        return self.chip(-step if slot % 2 else step)


def remote(src, dst, send_sem, recv_sem, device):
    return pltpu.make_async_remote_copy(
        src_ref=src, dst_ref=dst, send_sem=send_sem, recv_sem=recv_sem, device_id=device, device_id_type=MESH
    )


class Stream:
    def __init__(self, place, buf, share, parts, groups, send_s, ring_r, pair_r, twin_r):
        self.p, self.buf, self.parts, self.groups = place, buf, parts, groups
        self.ring_s, self.pair_s, self.twin_s = (send_s.at[n] for n in range(3))
        self.ring_r, self.pair_r, self.twin_r = ring_r, pair_r, twin_r
        width = buf.shape[1]
        tiles = width // LANE
        ring = max((tiles + 1) // 2, int(share * tiles)) if place.paired else tiles
        self.width = width
        self.ring_w = ring * LANE
        self.pair_w = width - self.ring_w
        self.ring_o = pl.multiple_of(place.side * self.pair_w, LANE) if place.paired else 0
        self.pair_o = pl.multiple_of((1 - place.side) * self.ring_w, LANE)
        self.give_o = pl.multiple_of(place.side * self.ring_w, LANE)
        self.block = buf.shape[0] // place.spans
        self.rows = self.block // parts
        self.last = place.chips // 2
        self.opposite = place.chips - 1
        self.handed = {0}

    def view(self, slot, part, cols):
        start = pl.multiple_of(slot * 2 * self.block + self.p.core * self.block + part * self.rows, self.rows)
        return self.buf.at[pl.ds(start, self.rows), cols]

    def bulk(self, rows, width):
        return self.buf.at[pl.ds(0, rows), pl.ds(0, width)]

    def ring_cols(self):
        return pl.ds(self.ring_o, self.ring_w)

    def slots(self, step):
        return (self.opposite,) if step == self.last else (2 * step - 1, 2 * step)

    def on(self, src_slot, dst_slot, part, way):
        cols = self.ring_cols()
        src, dst = self.view(src_slot, part, cols), self.view(dst_slot, part, cols)
        remote(src, dst, self.ring_s, self.ring_r.at[dst_slot, part], self.p.along(way)).start()

    def to_twin(self, slot, part, cols):
        view = self.view(slot, part, cols)
        group = [n for n, (lo, hi) in enumerate(self.groups) if lo <= slot < hi][0]
        remote(view, view, self.twin_s, self.twin_r.at[group], self.p.twin).start()

    def own(self, part):
        self.on(0, 1, part, 1)
        self.on(0, 2, part, -1)
        self.to_twin(0, part, pl.ds(0, self.width))

    def got(self, slot, part):
        view = self.view(slot, part, self.ring_cols())
        wait_bytes(view, self.ring_r.at[slot, part])

    def tick(self, step, part):
        if step == self.last:
            self.got(self.opposite, part)
        else:
            behind, ahead = self.slots(step)
            if step + 1 < self.last:
                self.got(behind, part)
                self.on(behind, behind + 2, part, 1)
                self.got(ahead, part)
                self.on(ahead, ahead + 2, part, -1)
            else:
                self.got(behind, part)
                self.got(ahead, part)
                self.on(behind + self.p.core, self.opposite, part, 1 - 2 * self.p.core)
        for slot in self.slots(step):
            if self.p.paired:
                view = self.view(slot, part, pl.ds(self.give_o, self.pair_w))
                remote(view, view, self.pair_s, self.pair_r.at[step, part], self.p.pair).start()
        for slot in self.slots(step):
            self.to_twin(slot, part, self.ring_cols())

    def pair_tick(self, step, part):
        slots = self.slots(step)
        if part == self.parts - 1:
            self.handed.update(slots)
        if not self.p.paired:
            return
        wait_bytes(self.bulk(len(slots) * self.rows, self.pair_w), self.pair_r.at[step, part])
        for slot in slots:
            self.to_twin(slot, part, pl.ds(self.pair_o, self.pair_w))

    def ready(self, group):
        lo, hi = self.groups[group]
        wait_bytes(self.bulk((hi - lo) * self.block, self.width), self.twin_r.at[group])

    def drain(self):
        rest = (self.p.chips - 1) * self.block
        wait_bytes(self.bulk(rest, self.ring_w), self.ring_s)
        if self.p.paired:
            wait_bytes(self.bulk(rest, self.pair_w), self.pair_s)
        wait_bytes(self.bulk(rest + self.block, self.width), self.twin_s)


def order(gate_up, down, last, late):
    def one(stream, step, part):
        while len(late) > PAIR_LAG:
            a, b, c = late.pop(0)
            a.pair_tick(b, c)
        stream.tick(step, part)
        late.append((stream, step, part))

    for step in range(1, last + DOWN_LAG + 1):
        for part in range(gate_up.parts):
            if step <= last:
                one(gate_up, step, part)
                yield
        for part in range(down.parts):
            if step == DOWN_LAG:
                down.own(part)
            elif step > DOWN_LAG:
                one(down, step - DOWN_LAG, part)
                yield
    while late:
        a, b, c = late.pop(0)
        a.pair_tick(b, c)


def all_to_all(place, src, dst, send_sem, recv_sem):
    chips = place.chips

    def body(t, _):
        step = chips // 2 + (1 - 2 * lax.rem(t, 2)) * lax.div(t + 1, 2)
        to = lax.rem(place.z + step, chips)
        for s, d, ss, rs in zip(src(to), dst(place.z), send_sem, recv_sem):
            remote(s, d, ss, rs, {"sp": 2 * to + place.core}).start()
        return 0

    lax.fori_loop(0, chips - 1, body, 0)


def wait_bytes(view, sem):
    pltpu.make_async_copy(view, view, sem).wait()


def layer(
    groups, spans, peers,
    q_hbm, k_hbm, v_hbm, g_hbm, ld_hbm, hg_hbm, wo_hbm, res_hbm, ng_hbm, gw_hbm, uw_hbm, dw_hbm, gt_hbm, ut_hbm,
    out_hbm,
    q_ref, k_ref, v_ref, g_ref, ld_ref, hg_ref, ng_ref, gt_ref, ut_ref, gu, dn, wo, res, st, st_twin, dec, dec_twin, st_send, st_recv, dec_send, dec_recv, in_send, in_recv, in_twin, inner, grow, mix, att, att_r,
    mid, nsend, nall, nperm, pre, halo_s, halo_r, hid, ff, ff_r, pair_sum, out_ref,
    load_sem, out_sem, twin_s, twin_r, a2a_s, a2a_r, tp_s, tp_r, mid_r, halo_ss, halo_rs,
    gu_s, gu_ring, gu_pair, gu_twin, dn_s, dn_ring, dn_pair, dn_twin,
):
    place = Place(groups, spans, peers)
    sp, tp, core = place.sp, place.tp, place.core
    length = q_hbm.shape[0]
    heads = q_hbm.shape[1] // HEAD
    combos = 2 * heads
    share = length // peers
    half_w = gw_hbm.shape[1]
    block = gw_hbm.shape[0]
    slots = place.chips
    scale = HEAD ** (-0.5)

    own_rows = pl.ds(pl.multiple_of(core * block, block), block)
    pairs = [
        (q_hbm, q_ref), (k_hbm, k_ref), (v_hbm, v_ref), (ld_hbm, ld_ref),
        (gw_hbm, gu.at[own_rows, pl.ds(0, half_w)]), (uw_hbm, gu.at[own_rows, pl.ds(half_w, half_w)]),
        (dw_hbm, dn.at[own_rows, :]), (g_hbm, g_ref), (hg_hbm, hg_ref), (wo_hbm, wo),
        (res_hbm.at[pl.ds(pl.multiple_of(tp * share, share), share), :], res), (ng_hbm, ng_ref), (gt_hbm, gt_ref),
        (ut_hbm, ut_ref),
    ]
    loads = [pltpu.make_async_copy(src, dst, load_sem.at[n]) for n, (src, dst) in enumerate(pairs)]
    for copy in loads:
        copy.start()

    barrier = pltpu.get_barrier_semaphore()

    def greet(step, _):
        pl.semaphore_signal(barrier, inc=1, device_id=place.along(step), device_id_type=MESH)
        return 0

    lax.fori_loop(1, place.chips, greet, 0)
    beside = {"sp": place.span(2 * core - 1)}
    for device in [place.twin, beside] + [{"tp": place.peer(step)} for step in range(1, peers)]:
        pl.semaphore_signal(barrier, inc=1, device_id=device, device_id_type=MESH)
    greeted = place.chips + peers
    if place.paired:
        pl.semaphore_signal(barrier, inc=1, device_id=place.pair, device_id_type=MESH)
        greeted += 1

    for copy in loads[:4]:
        copy.wait()
    row = lax.broadcasted_iota(jnp.int32, (HEAD, LANE), 0)
    lane = lax.broadcasted_iota(jnp.int32, (HEAD, LANE), 1)
    rates = [ld_ref[d, pl.ds(h, 1), :] for h in range(heads) for d in range(2)]
    sums = jnp.concatenate(rates + rates[: (-combos) % 8], axis=0) if combos % 8 else jnp.concatenate(rates, axis=0)
    s_lane = lax.broadcasted_iota(jnp.int32, sums.shape, 1)
    s_row = lax.broadcasted_iota(jnp.int32, sums.shape, 0)
    back = (s_row & 1) == 1
    shift = 1
    while shift < length:
        fwd = jnp.where(s_lane >= shift, pltpu.roll(sums, shift, 1), 0.0)
        bwd = jnp.where(s_lane < length - shift, pltpu.roll(sums, length - shift, 1), 0.0)
        sums = sums + jnp.where(back, bwd, fwd)
        shift *= 2
    chips = place.chips
    part = chips // 2
    rows = HEAD // part
    for h in range(heads):
        cols = pl.ds(h * HEAD, HEAD)
        q, k, v = q_ref[:, cols], k_ref[:, cols], v_ref[:, cols]
        v32 = v.astype(F32)
        scores = nt(q, k) * scale
        for d in range(2):
            m = 2 * h + d
            along_s = jnp.broadcast_to(sums[m : m + 1, :], (length, LANE))
            along_t = along_s.T
            seen = (row >= lane) if d == 0 else (row <= lane)
            decay = jnp.where(seen, jnp.exp(jnp.minimum(along_t - along_s, 0.0)), 0.0)
            inner[m] = nn((scores * decay).astype(BF16), v)
            grow[m] = jnp.exp(along_t) * scale
            total = along_t[length - 1 : length, :] if d == 0 else along_t[0:1, :]
            dec[m] = jnp.exp(total)
            faded = (v32 * jnp.exp(jnp.minimum(total - along_t, 0.0))).astype(BF16)
            st[m] = tn(k, faded).astype(BF16)

    early, cuts = groups_of(slots)
    gate_up = Stream(place, gu, GU_SHARE, GU_PARTS, early, gu_s, gu_ring, gu_pair, gu_twin)
    down = Stream(place, dn, DOWN_SHARE, DOWN_PARTS, cuts, dn_s, dn_ring, dn_pair, dn_twin)
    late = []
    ring = order(gate_up, down, place.chips // 2, late)

    def advance(n):
        for _ in range(n):
            next(ring, None)

    def ready(stream, group):
        wanted = set(range(*stream.groups[group]))
        while not stream.handed >= wanted:
            next(ring, None)
        stream.ready(group)

    for copy in loads[4:7]:
        copy.wait()
    pl.semaphore_wait(barrier, greeted)

    swaps = [
        remote(st, st_twin, twin_s.at[0], twin_r.at[0], place.twin),
        remote(dec, dec_twin, twin_s.at[1], twin_r.at[1], place.twin),
    ]
    for copy in swaps:
        copy.start()
    for part_no in range(OWN_FIRST):
        gate_up.own(part_no)
    for copy in swaps:
        copy.wait_recv()
    second = (core == 1).astype(F32)
    for d in range(2):
        m = 2 * core + d
        far = second if d == 0 else 1.0 - second
        mine, other = st[m].astype(F32), st_twin[m].astype(F32)
        my_dec, other_dec = dec[m], dec_twin[m]
        merged = mine * (far + (1.0 - far) * other_dec) + other * ((1.0 - far) + far * my_dec)
        st_send[pl.ds(d * part, part)] = merged.astype(BF16).reshape(part, rows, HEAD)
        dec_send[d] = my_dec * other_dec
    all_to_all(
        place,
        lambda to: (st_send.at[to], dec_send.at[lax.div(to, part)]),
        lambda me: (st_recv.at[me], dec_recv.at[me]),
        (a2a_s.at[0], a2a_s.at[1]),
        (a2a_r.at[0], a2a_r.at[1]),
    )
    for part_no in range(OWN_FIRST, GU_PARTS):
        gate_up.own(part_no)
    reverse = lax.div(place.z, part)
    st_recv[pl.ds(place.z, 1)] = st_send[pl.ds(place.z, 1)]
    dec_recv[pl.ds(place.z, 1)] = dec_send[pl.ds(reverse, 1)]
    advance(ADVANCE[0])
    others = pl.ds(0, chips - 1)
    wait_bytes(st_recv.at[others], a2a_r.at[0])
    wait_bytes(dec_recv.at[others], a2a_r.at[1])

    def scan(j, carry):
        at = j + reverse * (chips - 1 - 2 * j)
        in_send[at] = carry.astype(BF16)
        return carry * dec_recv[at] + st_recv[at].astype(F32)

    lax.fori_loop(0, chips, scan, jnp.zeros((rows, HEAD), F32))
    all_to_all(
        place, lambda to: (in_send.at[to],), lambda me: (in_recv.at[core, me],), (a2a_s.at[2],), (a2a_r.at[2],)
    )
    in_recv[core, pl.ds(place.z, 1)] = in_send[pl.ds(place.z, 1)]
    advance(ADVANCE[1])
    wait_bytes(in_recv.at[core, others], a2a_r.at[2])
    handover = remote(in_recv.at[core], in_twin, twin_s.at[2], twin_r.at[2], place.twin)
    handover.start()
    for copy in loads[7:]:
        copy.wait()
    advance(ADVANCE[2])
    handover.wait_recv()
    in_recv[1 - core] = in_twin[...]

    def normed_head(x):
        centre = x - jnp.mean(x, axis=1, keepdims=True)
        spread = jnp.mean(centre * centre, axis=1, keepdims=True)
        return centre * lax.rsqrt(spread + GROUP_EPS)

    for h in range(heads):
        cols = pl.ds(h * HEAD, HEAD)
        q = q_ref[:, cols]
        combined = None
        for d in range(2):
            m = 2 * h + d
            state = in_recv[h, pl.ds(d * part, part)].reshape(HEAD, HEAD).astype(F32)
            far = second if d == 0 else 1.0 - second
            state = state * (far * dec_twin[m] + (1.0 - far)) + far * st_twin[m].astype(F32)
            state = state.astype(BF16)
            term = normed_head(inner[m] + grow[m] * nn(q, state)) * hg_ref[pl.ds(d, 1), cols]
            combined = term if combined is None else combined + term
        gate = g_ref[:, cols].astype(F32)
        mix[:, cols] = (gate / (1.0 + jnp.exp(-gate)) * combined).astype(BF16)

    width = wo.shape[1]
    tile = min(512, width)
    for n in range(width // tile):
        cols = pl.ds(n * tile, tile)
        att[:, cols] = nn(mix[...], wo[:, cols]).astype(BF16)

    def peer_rows(j):
        return pl.ds(pl.multiple_of(j * share, share), share)

    def to_peers(src, dst, s, r):
        for step in range(1, peers):
            remote(src(place.peer(step)), dst(step), s, r, {"tp": place.peer(step)}).start()

    foreign = pl.ds(0, (peers - 1) * share)
    to_peers(lambda j: att.at[peer_rows(j), :], lambda step: att_r.at[step - 1], tp_s.at[0], tp_r.at[0])
    advance(ADVANCE[3])
    wait_bytes(att_r, tp_r.at[0])
    total = att[peer_rows(tp), :].astype(F32)
    for step in range(1, peers):
        total = total + att_r[step - 1].astype(F32)
    middle = (res[...].astype(F32) + total).astype(BF16)
    mid[...] = middle
    values = middle.astype(F32)
    multiplier = lax.rsqrt(jnp.mean(values * values, axis=1, keepdims=True) + NORM_EPS)
    normed = (values * multiplier * ng_ref[...].astype(F32).reshape(1, -1)).astype(BF16)
    nsend[...] = normed
    nall[peer_rows(tp), :] = normed
    to_peers(lambda j: nsend, lambda step: nall.at[peer_rows(tp), :], tp_s.at[1], tp_r.at[1])
    advance(ADVANCE[4])
    wait_bytes(nall.at[foreign, :], tp_r.at[1])
    halo_s[0] = nall[0:1, :].astype(F32)
    halo_s[1] = nall[length - 1 : length, :].astype(F32)
    before, after = {"sp": place.span(-1)}, {"sp": place.span(1)}
    halos = [
        remote(halo_s.at[0], halo_r.at[1], halo_ss.at[0], halo_rs.at[1], before),
        remote(halo_s.at[1], halo_r.at[0], halo_ss.at[1], halo_rs.at[0], after),
    ]
    for copy in halos:
        copy.start()
    for slot in range(slots):
        start = pl.multiple_of(place.slot_chip(slot) * LANE, LANE)
        nperm[0:length, pl.ds(slot * LANE, LANE)] = nall[:, pl.ds(start, LANE)]
    advance(ADVANCE[5])
    for copy in halos:
        copy.wait_recv()
    rim_row = lax.broadcasted_iota(jnp.int32, (RIM, LANE), 0)
    not_first = (sp > 0).astype(F32)
    not_last = (sp < spans - 1).astype(F32)
    for slot in range(slots):
        cols = pl.ds(pl.multiple_of(place.slot_chip(slot) * LANE, LANE), LANE)
        rim = jnp.where(rim_row == 0, halo_r[0, :, cols] * not_first, 0.0)
        rim = jnp.where(rim_row == 1, halo_r[1, :, cols] * not_last, rim)
        nperm[pl.ds(length, RIM), pl.ds(slot * LANE, LANE)] = rim.astype(BF16)

    ready(gate_up, 0)
    n_tile = 256 if (2 * half_w) % 256 == 0 else 128
    count = 2 * half_w // n_tile
    split_at = early[0][1] * 2 * block
    head_k, tail_k = pl.ds(0, split_at), pl.ds(split_at, spans * block - split_at)

    def tile_cols(n):
        return pl.ds(pl.multiple_of(n * n_tile, n_tile), n_tile)

    def project(n, _):
        pre[:, tile_cols(n)] = nn(nperm[:, head_k], gu[head_k, tile_cols(n)])
        return 0

    thirds = [count * n // 3 for n in range(4)]
    for lo, hi in zip(thirds[:-1], thirds[1:]):
        lax.fori_loop(lo, hi, project, 0)
        advance(ADVANCE[6])
    ready(gate_up, 1)

    def project_rest(n, _):
        total = pre[:, tile_cols(n)] + nn(nperm[:, tail_k], gu[tail_k, tile_cols(n)])
        pre[:, tile_cols(n)] = total.astype(BF16).astype(F32)
        return 0

    lax.fori_loop(0, count // 2, project_rest, 0)
    advance(ADVANCE[7])
    lax.fori_loop(count // 2, count, project_rest, 0)
    advance(ADVANCE[8])
    def conv(n, _):
        results = []
        for base, taps in ((0, gt_ref), (half_w, ut_ref)):
            cols = pl.ds(pl.multiple_of(base + n * LANE, LANE), LANE)
            x = pre[0:length, cols]
            above = jnp.where(row == 0, pre[pl.ds(length, 1), cols], pltpu.roll(x, 1, 0))
            below = jnp.where(row == length - 1, pre[pl.ds(length + 1, 1), cols], pltpu.roll(x, length - 1, 0))
            t = taps[:, pl.ds(pl.multiple_of(n * LANE, LANE), LANE)].astype(F32)
            results.append(t[0:1] * above + t[1:2] * x + t[2:3] * below)
        gate, up = results
        hid[:, pl.ds(pl.multiple_of(n * LANE, LANE), LANE)] = (gate / (1.0 + jnp.exp(-gate)) * up).astype(BF16)
        return 0

    lax.fori_loop(0, half_w // LANE, conv, 0)
    advance(ADVANCE[9])

    right, left = {"tp": place.peer(1)}, {"tp": place.peer(peers - 1)}

    def sides(lo, hi):
        middle = (lo + hi) // 2
        first, second = pl.ds(lo * LANE, (middle - lo) * LANE), pl.ds(middle * LANE, (hi - middle) * LANE)
        return (0, first, second, right, place.peer(1)), (1, second, first, left, place.peer(peers - 1))

    def around_first(n, lo, hi):
        for plane, shared, alone, device, to in sides(lo, hi):
            far = ff.at[peer_rows(place.peer(2)), shared]
            remote(far, ff_r.at[2, :, shared], tp_s.at[2 + n], mid_r.at[n], device).start()
            near = ff.at[peer_rows(to), alone]
            remote(near, ff_r.at[plane, :, alone], tp_s.at[2 + n], tp_r.at[2 + n], device).start()

    def around_second(n, lo, hi):
        wait_bytes(ff_r.at[2, :, pl.ds(lo * LANE, (hi - lo) * LANE)], mid_r.at[n])
        for plane, shared, alone, device, to in sides(lo, hi):
            total = ff[peer_rows(to), shared].astype(F32) + ff_r[2, :, shared].astype(F32)
            pair_sum[plane, :, shared] = total.astype(BF16)
            remote(
                pair_sum.at[plane, :, shared], ff_r.at[plane, :, shared], tp_s.at[2 + n], tp_r.at[2 + n], device
            ).start()

    for part_no, (lo, hi) in enumerate(cuts):
        ready(down, part_no)

        def project_down(n, _):
            rows_ = pl.ds(pl.multiple_of(n * 2 * LANE, 2 * LANE), 2 * LANE)
            ff[:, rows_] = nt(hid[...], dn[rows_, :]).astype(BF16)
            return 0

        lax.fori_loop(lo // 2, hi // 2, project_down, 0)
        cols = pl.ds(lo * LANE, (hi - lo) * LANE)
        if AROUND and peers == 4:
            around_first(part_no, lo, hi)
        else:
            to_peers(
                lambda j: ff.at[peer_rows(j), cols],
                lambda step: ff_r.at[step - 1, :, cols],
                tp_s.at[2 + part_no],
                tp_r.at[2 + part_no],
            )
    if AROUND and peers == 4:
        for part_no, (lo, hi) in enumerate(cuts):
            around_second(part_no, lo, hi)
    for part_no, (lo, hi) in enumerate(cuts):
        cols = pl.ds(lo * LANE, (hi - lo) * LANE)
        arriving = 2 if AROUND and peers == 4 else peers - 1
        wait_bytes(ff_r.at[pl.ds(0, arriving), :, cols], tp_r.at[2 + part_no])
        for slot in range(lo, hi):
            held = pl.ds(slot * LANE, LANE)
            home = pl.ds(pl.multiple_of(place.slot_chip(slot) * LANE, LANE), LANE)
            total = ff[peer_rows(tp), held].astype(F32)
            for step in range(arriving):
                total = total + ff_r[step, :, held].astype(F32)
            out_ref[:, home] = (mid[:, home].astype(F32) + total).astype(BF16)
        for slot in range(lo, hi):
            home = pl.ds(pl.multiple_of(place.slot_chip(slot) * LANE, LANE), LANE)
            pltpu.make_async_copy(out_ref.at[:, home], out_hbm.at[:, home], out_sem).start()

    advance(10_000)
    for copy in halos + swaps + [handover]:
        copy.wait_send()
    for n in range(2):
        wait_bytes(att_r, tp_s.at[n])
    for n, (lo, hi) in enumerate(cuts):
        wait_bytes(ff_r.at[:, :, pl.ds(lo * LANE, (hi - lo) * LANE)], tp_s.at[2 + n])
    wait_bytes(st_send.at[others], a2a_s.at[0])
    wait_bytes(dec_recv.at[others], a2a_s.at[1])
    wait_bytes(in_send.at[others], a2a_s.at[2])
    gate_up.drain()
    down.drain()
    wait_bytes(out_ref, out_sem)


PAIRED = True
OWN_FIRST = 1
AROUND = False
GU_SHARE = 0.69
DOWN_SHARE = 0.66
RIM = 16
EARLY = 1
PAIR_LAG = 2
DOWN_LAG = 1
GU_PARTS = 2
DOWN_PARTS = 2
ADVANCE = (4, 7, 1, 5, 5, 2, 1, 1, 0, 1)


def solution(mesh):
    groups, spans, peers = mesh.shape["grp"], mesh.shape["sp"], mesh.shape["tp"]
    rows_, cols_ = ("grp", "sp"), "tp"
    placed = (
        P(rows_, cols_), P(rows_, cols_), P(rows_, cols_), P(rows_, cols_), P(None, cols_, rows_), P(None, cols_),
        P(cols_, None), P(rows_, None), P(), P("sp", cols_), P("sp", cols_), P("sp", cols_), P(None, cols_),
        P(None, cols_),
    )

    def shards(q, k, v, g, ld, hg, wo, res, ng, gw, uw, dw, gt, ut):
        length = q.shape[0]
        heads = q.shape[1] // HEAD
        combos = 2 * heads
        share = length // peers
        block, half_w = gw.shape
        width = wo.shape[1]
        chips = spans // 2
        packet = 2 * HEAD // chips
        dma = pltpu.SemaphoreType.DMA
        hbm = pl.BlockSpec(memory_space=pltpu.HBM)
        scratch = [pltpu.VMEM(a.shape, a.dtype) for a in (q, k, v, g, ld, hg, ng, gt, ut)] + [
            pltpu.VMEM((spans * block, 2 * half_w), BF16),
            pltpu.VMEM((spans * block, half_w), BF16),
            pltpu.VMEM(wo.shape, BF16),
            pltpu.VMEM((share, width), BF16),
            pltpu.VMEM((combos, HEAD, HEAD), BF16),
            pltpu.VMEM((combos, HEAD, HEAD), BF16),
            pltpu.VMEM((combos, 1, LANE), F32),
            pltpu.VMEM((combos, 1, LANE), F32),
            pltpu.VMEM((chips, packet, HEAD), BF16),
            pltpu.VMEM((chips, packet, HEAD), BF16),
            pltpu.VMEM((2, 1, LANE), F32),
            pltpu.VMEM((chips, 1, LANE), F32),
            pltpu.VMEM((chips, packet, HEAD), BF16),
            pltpu.VMEM((2, chips, packet, HEAD), BF16),
            pltpu.VMEM((chips, packet, HEAD), BF16),
            pltpu.VMEM((combos, length, HEAD), F32),
            pltpu.VMEM((combos, length, HEAD), F32),
            pltpu.VMEM((length, heads * HEAD), BF16),
            pltpu.VMEM((length, width), BF16),
            pltpu.VMEM((peers - 1, share, width), BF16),
            pltpu.VMEM((share, width), BF16),
            pltpu.VMEM((share, width), BF16),
            pltpu.VMEM((length, width), BF16),
            pltpu.VMEM((length + RIM, width), BF16),
            pltpu.VMEM((length + RIM, 2 * half_w), F32),
            pltpu.VMEM((2, 1, width), F32),
            pltpu.VMEM((2, 1, width), F32),
            pltpu.VMEM((length, half_w), BF16),
            pltpu.VMEM((length, width), BF16),
            pltpu.VMEM((peers - 1, share, width), BF16),
            pltpu.VMEM((2, share, width), BF16),
            pltpu.VMEM((share, width), BF16),
            dma((14,)), dma, dma((3,)), dma((3,)), dma((3,)), dma((3,)), dma((6,)), dma((6,)), dma((4,)), dma((2,)), dma((2,)),
        ]
        for parts, held in zip((GU_PARTS, DOWN_PARTS), groups_of(chips)):
            scratch += [dma((3,)), dma((chips, parts)), dma((chips // 2 + 1, parts)), dma((len(held),))]
        return pl.pallas_call(
            functools.partial(layer, groups, spans, peers),
            name="layer",
            out_shape=jax.ShapeDtypeStruct((share, width), BF16),
            in_specs=[hbm] * 14,
            out_specs=hbm,
            scratch_shapes=scratch,
            compiler_params=pltpu.CompilerParams(
                collective_id=0, has_side_effects=True, vmem_limit_bytes=67_043_328
            ),
        )(q, k, v, g, ld, hg, wo, res, ng, gw, uw, dw, gt, ut)

    return jax.shard_map(shards, mesh=mesh, in_specs=placed, out_specs=P(("grp", "sp", "tp"), None), check_vma=False)
```

```python
import functools

import jax
import jax.numpy as jnp
from jax import lax
from jax.experimental import pallas as pl
from jax.experimental.pallas import tpu as pltpu
from jax.sharding import PartitionSpec as P

HEAD = 128
LANE = 128
GROUP_EPS = 1e-05
NORM_EPS = 1e-06
MESH = pl.DeviceIdType.MESH
F32 = jnp.float32
BF16 = jnp.bfloat16


def nt(a, b):
    return lax.dot_general(a, b, (((1,), (1,)), ((), ())), preferred_element_type=F32)


def tn(a, b):
    return lax.dot_general(a, b, (((0,), (0,)), ((), ())), preferred_element_type=F32)


def nn(a, b):
    return jnp.dot(a, b, preferred_element_type=F32)


def groups_of(slots):
    early = slots - EARLY
    cuts = sorted({0, slots // 2, slots - 4, slots - 2, slots})
    return [(0, early), (early, slots)], list(zip(cuts[:-1], cuts[1:]))


class Place:
    def __init__(self, groups, spans, peers):
        self.spans, self.peers, self.chips = spans, peers, spans // 2
        self.sp = lax.axis_index("sp")
        self.tp = lax.axis_index("tp")
        self.core = lax.rem(self.sp, 2)
        self.z = lax.div(self.sp, 2)
        self.paired = PAIRED and groups % 2 == 0
        grp = lax.axis_index("grp")
        self.side = lax.rem(grp, 2)
        self.pair = {"grp": grp + 1 - 2 * self.side}
        self.twin = {"sp": self.sp + 1 - 2 * self.core}

    def chip(self, step):
        return lax.rem(self.z + step + self.chips, self.chips)

    def along(self, step):
        return {"sp": 2 * self.chip(step) + self.core}

    def span(self, step):
        return lax.rem(self.sp + step + self.spans, self.spans)

    def peer(self, step):
        return lax.rem(self.tp + step, self.peers)

    def slot_chip(self, slot):
        step = (slot + 1) // 2
        return self.chip(-step if slot % 2 else step)


def remote(src, dst, send_sem, recv_sem, device):
    return pltpu.make_async_remote_copy(
        src_ref=src, dst_ref=dst, send_sem=send_sem, recv_sem=recv_sem, device_id=device, device_id_type=MESH
    )


class Stream:
    def __init__(self, place, buf, share, parts, groups, send_s, ring_r, pair_r, twin_r):
        self.p, self.buf, self.parts, self.groups = place, buf, parts, groups
        self.ring_s, self.pair_s, self.twin_s = (send_s.at[n] for n in range(3))
        self.ring_r, self.pair_r, self.twin_r = ring_r, pair_r, twin_r
        width = buf.shape[1]
        tiles = width // LANE
        ring = max((tiles + 1) // 2, int(share * tiles)) if place.paired else tiles
        self.width = width
        self.ring_w = ring * LANE
        self.pair_w = width - self.ring_w
        self.ring_o = pl.multiple_of(place.side * self.pair_w, LANE) if place.paired else 0
        self.pair_o = pl.multiple_of((1 - place.side) * self.ring_w, LANE)
        self.give_o = pl.multiple_of(place.side * self.ring_w, LANE)
        self.block = buf.shape[0] // place.spans
        self.rows = self.block // parts
        self.last = place.chips // 2
        self.opposite = place.chips - 1
        self.handed = {0}

    def view(self, slot, part, cols):
        start = pl.multiple_of(slot * 2 * self.block + self.p.core * self.block + part * self.rows, self.rows)
        return self.buf.at[pl.ds(start, self.rows), cols]

    def whole(self, slot, cols):
        start = pl.multiple_of(slot * 2 * self.block + self.p.core * self.block, self.block)
        return self.buf.at[pl.ds(start, self.block), cols]

    def bulk(self, rows, width):
        return self.buf.at[pl.ds(0, rows), pl.ds(0, width)]

    def ring_cols(self):
        return pl.ds(self.ring_o, self.ring_w)

    def slots(self, step):
        return (self.opposite,) if step == self.last else (2 * step - 1, 2 * step)

    def on(self, src_slot, dst_slot, part, way):
        cols = self.ring_cols()
        src, dst = self.view(src_slot, part, cols), self.view(dst_slot, part, cols)
        remote(src, dst, self.ring_s, self.ring_r.at[dst_slot, part], self.p.along(way)).start()

    def to_twin(self, slot, cols):
        view = self.whole(slot, cols)
        group = [n for n, (lo, hi) in enumerate(self.groups) if lo <= slot < hi][0]
        remote(view, view, self.twin_s, self.twin_r.at[group], self.p.twin).start()

    def own(self, part):
        self.on(0, 1, part, 1)
        self.on(0, 2, part, -1)
        if part == self.parts - 1:
            self.to_twin(0, pl.ds(0, self.width))

    def got(self, slot, part):
        view = self.view(slot, part, self.ring_cols())
        wait_bytes(view, self.ring_r.at[slot, part])

    def tick(self, step, part):
        if step == self.last:
            self.got(self.opposite, part)
        else:
            behind, ahead = self.slots(step)
            if step + 1 < self.last:
                self.got(behind, part)
                self.on(behind, behind + 2, part, 1)
                self.got(ahead, part)
                self.on(ahead, ahead + 2, part, -1)
            else:
                self.got(behind, part)
                self.got(ahead, part)
                self.on(behind + self.p.core, self.opposite, part, 1 - 2 * self.p.core)
        if part < self.parts - 1:
            return
        for slot in self.slots(step):
            if self.p.paired:
                view = self.whole(slot, pl.ds(self.give_o, self.pair_w))
                remote(view, view, self.pair_s, self.pair_r.at[step], self.p.pair).start()
        for slot in self.slots(step):
            self.to_twin(slot, self.ring_cols())

    def pair_tick(self, step, part):
        if part < self.parts - 1:
            return
        slots = self.slots(step)
        self.handed.update(slots)
        if not self.p.paired:
            return
        wait_bytes(self.bulk(len(slots) * self.block, self.pair_w), self.pair_r.at[step])
        for slot in slots:
            self.to_twin(slot, pl.ds(self.pair_o, self.pair_w))

    def ready(self, group):
        lo, hi = self.groups[group]
        wait_bytes(self.bulk((hi - lo) * self.block, self.width), self.twin_r.at[group])

    def drain(self):
        rest = (self.p.chips - 1) * self.block
        wait_bytes(self.bulk(rest, self.ring_w), self.ring_s)
        if self.p.paired:
            wait_bytes(self.bulk(rest, self.pair_w), self.pair_s)
        wait_bytes(self.bulk(rest + self.block, self.width), self.twin_s)


def order(gate_up, down, last, late):
    def one(stream, step, part):
        while len(late) > PAIR_LAG:
            a, b, c = late.pop(0)
            a.pair_tick(b, c)
        stream.tick(step, part)
        late.append((stream, step, part))

    for step in range(1, last + DOWN_LAG + 1):
        for part in range(gate_up.parts):
            if step <= last:
                one(gate_up, step, part)
                yield
        for part in range(down.parts):
            if step == DOWN_LAG:
                down.own(part)
            elif step > DOWN_LAG:
                one(down, step - DOWN_LAG, part)
                yield
    while late:
        a, b, c = late.pop(0)
        a.pair_tick(b, c)


def all_to_all(place, src, dst, send_sem, recv_sem):
    chips = place.chips

    def body(t, _):
        step = chips // 2 + (1 - 2 * lax.rem(t, 2)) * lax.div(t + 1, 2)
        to = lax.rem(place.z + step, chips)
        for s, d, ss, rs in zip(src(to), dst(place.z), send_sem, recv_sem):
            remote(s, d, ss, rs, {"sp": 2 * to + place.core}).start()
        return 0

    lax.fori_loop(0, chips - 1, body, 0)


def wait_bytes(view, sem):
    pltpu.make_async_copy(view, view, sem).wait()


def layer(
    groups, spans, peers,
    q_hbm, k_hbm, v_hbm, g_hbm, ld_hbm, hg_hbm, wo_hbm, res_hbm, ng_hbm, gw_hbm, uw_hbm, dw_hbm, gt_hbm, ut_hbm,
    out_hbm,
    q_ref, k_ref, v_ref, g_ref, ld_ref, hg_ref, ng_ref, gt_ref, ut_ref, gu, dn, wo, res, st, st_twin, dec, dec_twin, st_send, st_recv, dec_send, dec_recv, in_send, in_recv, in_twin, inner, grow, mix, att, att_r,
    mid, nsend, nall, nperm, pre, halo_s, halo_r, hid, ff, ff_r, pair_sum, out_ref,
    load_sem, out_sem, twin_s, twin_r, a2a_s, a2a_r, tp_s, tp_r, mid_r, halo_ss, halo_rs,
    gu_s, gu_ring, gu_pair, gu_twin, dn_s, dn_ring, dn_pair, dn_twin,
):
    place = Place(groups, spans, peers)
    sp, tp, core = place.sp, place.tp, place.core
    length = q_hbm.shape[0]
    heads = q_hbm.shape[1] // HEAD
    combos = 2 * heads
    share = length // peers
    half_w = gw_hbm.shape[1]
    block = gw_hbm.shape[0]
    slots = place.chips
    scale = HEAD ** (-0.5)

    own_rows = pl.ds(pl.multiple_of(core * block, block), block)
    pairs = [
        (q_hbm, q_ref), (k_hbm, k_ref), (v_hbm, v_ref), (ld_hbm, ld_ref),
        (gw_hbm, gu.at[own_rows, pl.ds(0, half_w)]), (uw_hbm, gu.at[own_rows, pl.ds(half_w, half_w)]),
        (dw_hbm, dn.at[own_rows, :]), (g_hbm, g_ref), (hg_hbm, hg_ref), (wo_hbm, wo),
        (res_hbm.at[pl.ds(pl.multiple_of(tp * share, share), share), :], res), (ng_hbm, ng_ref), (gt_hbm, gt_ref),
        (ut_hbm, ut_ref),
    ]
    loads = [pltpu.make_async_copy(src, dst, load_sem.at[n]) for n, (src, dst) in enumerate(pairs)]
    for copy in loads:
        copy.start()

    barrier = pltpu.get_barrier_semaphore()

    def greet(step, _):
        pl.semaphore_signal(barrier, inc=1, device_id=place.along(step), device_id_type=MESH)
        return 0

    lax.fori_loop(1, place.chips, greet, 0)
    beside = {"sp": place.span(2 * core - 1)}
    for device in [place.twin, beside] + [{"tp": place.peer(step)} for step in range(1, peers)]:
        pl.semaphore_signal(barrier, inc=1, device_id=device, device_id_type=MESH)
    greeted = place.chips + peers
    if place.paired:
        pl.semaphore_signal(barrier, inc=1, device_id=place.pair, device_id_type=MESH)
        greeted += 1

    for copy in loads[:4]:
        copy.wait()
    row = lax.broadcasted_iota(jnp.int32, (HEAD, LANE), 0)
    lane = lax.broadcasted_iota(jnp.int32, (HEAD, LANE), 1)
    rates = [ld_ref[d, pl.ds(h, 1), :] for h in range(heads) for d in range(2)]
    sums = jnp.concatenate(rates + rates[: (-combos) % 8], axis=0) if combos % 8 else jnp.concatenate(rates, axis=0)
    s_lane = lax.broadcasted_iota(jnp.int32, sums.shape, 1)
    s_row = lax.broadcasted_iota(jnp.int32, sums.shape, 0)
    back = (s_row & 1) == 1
    shift = 1
    while shift < length:
        fwd = jnp.where(s_lane >= shift, pltpu.roll(sums, shift, 1), 0.0)
        bwd = jnp.where(s_lane < length - shift, pltpu.roll(sums, length - shift, 1), 0.0)
        sums = sums + jnp.where(back, bwd, fwd)
        shift *= 2
    chips = place.chips
    part = chips // 2
    rows = HEAD // part
    for h in range(heads):
        cols = pl.ds(h * HEAD, HEAD)
        q, k, v = q_ref[:, cols], k_ref[:, cols], v_ref[:, cols]
        v32 = v.astype(F32)
        scores = nt(q, k) * scale
        for d in range(2):
            m = 2 * h + d
            along_s = jnp.broadcast_to(sums[m : m + 1, :], (length, LANE))
            along_t = along_s.T
            seen = (row >= lane) if d == 0 else (row <= lane)
            decay = jnp.where(seen, jnp.exp(jnp.minimum(along_t - along_s, 0.0)), 0.0)
            inner[m] = nn((scores * decay).astype(BF16), v)
            grow[m] = jnp.exp(along_t) * scale
            total = along_t[length - 1 : length, :] if d == 0 else along_t[0:1, :]
            dec[m] = jnp.exp(total)
            faded = (v32 * jnp.exp(jnp.minimum(total - along_t, 0.0))).astype(BF16)
            st[m] = tn(k, faded).astype(BF16)

    early, cuts = groups_of(slots)
    gate_up = Stream(place, gu, GU_SHARE, GU_PARTS, early, gu_s, gu_ring, gu_pair, gu_twin)
    down = Stream(place, dn, DOWN_SHARE, DOWN_PARTS, cuts, dn_s, dn_ring, dn_pair, dn_twin)
    late = []
    ring = order(gate_up, down, place.chips // 2, late)

    def advance(n):
        for _ in range(n):
            next(ring, None)

    def ready(stream, group):
        wanted = set(range(*stream.groups[group]))
        while not stream.handed >= wanted:
            next(ring, None)
        stream.ready(group)

    for copy in loads[4:7]:
        copy.wait()
    pl.semaphore_wait(barrier, greeted)

    swaps = [
        remote(st, st_twin, twin_s.at[0], twin_r.at[0], place.twin),
        remote(dec, dec_twin, twin_s.at[1], twin_r.at[1], place.twin),
    ]
    for copy in swaps:
        copy.start()
    for part_no in range(OWN_FIRST):
        gate_up.own(part_no)
    for copy in swaps:
        copy.wait_recv()
    second = (core == 1).astype(F32)
    for d in range(2):
        m = 2 * core + d
        far = second if d == 0 else 1.0 - second
        mine, other = st[m].astype(F32), st_twin[m].astype(F32)
        my_dec, other_dec = dec[m], dec_twin[m]
        merged = mine * (far + (1.0 - far) * other_dec) + other * ((1.0 - far) + far * my_dec)
        st_send[pl.ds(d * part, part)] = merged.astype(BF16).reshape(part, rows, HEAD)
        dec_send[d] = my_dec * other_dec
    all_to_all(
        place,
        lambda to: (st_send.at[to], dec_send.at[lax.div(to, part)]),
        lambda me: (st_recv.at[me], dec_recv.at[me]),
        (a2a_s.at[0], a2a_s.at[1]),
        (a2a_r.at[0], a2a_r.at[1]),
    )
    for part_no in range(OWN_FIRST, GU_PARTS):
        gate_up.own(part_no)
    reverse = lax.div(place.z, part)
    st_recv[pl.ds(place.z, 1)] = st_send[pl.ds(place.z, 1)]
    dec_recv[pl.ds(place.z, 1)] = dec_send[pl.ds(reverse, 1)]
    advance(ADVANCE[0])
    others = pl.ds(0, chips - 1)
    wait_bytes(st_recv.at[others], a2a_r.at[0])
    wait_bytes(dec_recv.at[others], a2a_r.at[1])

    def scan(j, carry):
        at = j + reverse * (chips - 1 - 2 * j)
        in_send[at] = carry.astype(BF16)
        return carry * dec_recv[at] + st_recv[at].astype(F32)

    lax.fori_loop(0, chips, scan, jnp.zeros((rows, HEAD), F32))
    all_to_all(
        place, lambda to: (in_send.at[to],), lambda me: (in_recv.at[core, me],), (a2a_s.at[2],), (a2a_r.at[2],)
    )
    in_recv[core, pl.ds(place.z, 1)] = in_send[pl.ds(place.z, 1)]
    advance(ADVANCE[1])
    wait_bytes(in_recv.at[core, others], a2a_r.at[2])
    handover = remote(in_recv.at[core], in_twin, twin_s.at[2], twin_r.at[2], place.twin)
    handover.start()
    for copy in loads[7:]:
        copy.wait()
    advance(ADVANCE[2])
    handover.wait_recv()
    in_recv[1 - core] = in_twin[...]

    def normed_head(x):
        centre = x - jnp.mean(x, axis=1, keepdims=True)
        spread = jnp.mean(centre * centre, axis=1, keepdims=True)
        return centre * lax.rsqrt(spread + GROUP_EPS)

    for h in range(heads):
        cols = pl.ds(h * HEAD, HEAD)
        q = q_ref[:, cols]
        combined = None
        for d in range(2):
            m = 2 * h + d
            state = in_recv[h, pl.ds(d * part, part)].reshape(HEAD, HEAD).astype(F32)
            far = second if d == 0 else 1.0 - second
            state = state * (far * dec_twin[m] + (1.0 - far)) + far * st_twin[m].astype(F32)
            state = state.astype(BF16)
            term = normed_head(inner[m] + grow[m] * nn(q, state)) * hg_ref[pl.ds(d, 1), cols]
            combined = term if combined is None else combined + term
        gate = g_ref[:, cols].astype(F32)
        mix[:, cols] = (gate / (1.0 + jnp.exp(-gate)) * combined).astype(BF16)

    width = wo.shape[1]
    tile = min(512, width)
    for n in range(width // tile):
        cols = pl.ds(n * tile, tile)
        att[:, cols] = nn(mix[...], wo[:, cols]).astype(BF16)

    def peer_rows(j):
        return pl.ds(pl.multiple_of(j * share, share), share)

    def to_peers(src, dst, s, r):
        for step in range(1, peers):
            remote(src(place.peer(step)), dst(step), s, r, {"tp": place.peer(step)}).start()

    foreign = pl.ds(0, (peers - 1) * share)
    to_peers(lambda j: att.at[peer_rows(j), :], lambda step: att_r.at[step - 1], tp_s.at[0], tp_r.at[0])
    advance(ADVANCE[3])
    wait_bytes(att_r, tp_r.at[0])
    total = att[peer_rows(tp), :].astype(F32)
    for step in range(1, peers):
        total = total + att_r[step - 1].astype(F32)
    middle = (res[...].astype(F32) + total).astype(BF16)
    mid[...] = middle
    values = middle.astype(F32)
    multiplier = lax.rsqrt(jnp.mean(values * values, axis=1, keepdims=True) + NORM_EPS)
    normed = (values * multiplier * ng_ref[...].astype(F32).reshape(1, -1)).astype(BF16)
    nsend[...] = normed
    nall[peer_rows(tp), :] = normed
    to_peers(lambda j: nsend, lambda step: nall.at[peer_rows(tp), :], tp_s.at[1], tp_r.at[1])
    advance(ADVANCE[4])
    wait_bytes(nall.at[foreign, :], tp_r.at[1])
    halo_s[0] = nall[0:1, :].astype(F32)
    halo_s[1] = nall[length - 1 : length, :].astype(F32)
    before, after = {"sp": place.span(-1)}, {"sp": place.span(1)}
    halos = [
        remote(halo_s.at[0], halo_r.at[1], halo_ss.at[0], halo_rs.at[1], before),
        remote(halo_s.at[1], halo_r.at[0], halo_ss.at[1], halo_rs.at[0], after),
    ]
    for copy in halos:
        copy.start()
    for slot in range(slots):
        start = pl.multiple_of(place.slot_chip(slot) * LANE, LANE)
        nperm[0:length, pl.ds(slot * LANE, LANE)] = nall[:, pl.ds(start, LANE)]
    advance(ADVANCE[5])
    for copy in halos:
        copy.wait_recv()
    rim_row = lax.broadcasted_iota(jnp.int32, (RIM, LANE), 0)
    not_first = (sp > 0).astype(F32)
    not_last = (sp < spans - 1).astype(F32)
    for slot in range(slots):
        cols = pl.ds(pl.multiple_of(place.slot_chip(slot) * LANE, LANE), LANE)
        rim = jnp.where(rim_row == 0, halo_r[0, :, cols] * not_first, 0.0)
        rim = jnp.where(rim_row == 1, halo_r[1, :, cols] * not_last, rim)
        nperm[pl.ds(length, RIM), pl.ds(slot * LANE, LANE)] = rim.astype(BF16)

    ready(gate_up, 0)
    n_tile = 256 if (2 * half_w) % 256 == 0 else 128
    count = 2 * half_w // n_tile
    split_at = early[0][1] * 2 * block
    head_k, tail_k = pl.ds(0, split_at), pl.ds(split_at, spans * block - split_at)

    def tile_cols(n):
        return pl.ds(pl.multiple_of(n * n_tile, n_tile), n_tile)

    def project(n, _):
        pre[:, tile_cols(n)] = nn(nperm[:, head_k], gu[head_k, tile_cols(n)])
        return 0

    thirds = [count * n // 3 for n in range(4)]
    for lo, hi in zip(thirds[:-1], thirds[1:]):
        lax.fori_loop(lo, hi, project, 0)
        advance(ADVANCE[6])
    ready(gate_up, 1)

    def project_rest(n, _):
        total = pre[:, tile_cols(n)] + nn(nperm[:, tail_k], gu[tail_k, tile_cols(n)])
        pre[:, tile_cols(n)] = total.astype(BF16).astype(F32)
        return 0

    lax.fori_loop(0, count // 2, project_rest, 0)
    advance(ADVANCE[7])
    lax.fori_loop(count // 2, count, project_rest, 0)
    advance(ADVANCE[8])
    def conv(n, _):
        results = []
        for base, taps in ((0, gt_ref), (half_w, ut_ref)):
            cols = pl.ds(pl.multiple_of(base + n * LANE, LANE), LANE)
            x = pre[0:length, cols]
            above = jnp.where(row == 0, pre[pl.ds(length, 1), cols], pltpu.roll(x, 1, 0))
            below = jnp.where(row == length - 1, pre[pl.ds(length + 1, 1), cols], pltpu.roll(x, length - 1, 0))
            t = taps[:, pl.ds(pl.multiple_of(n * LANE, LANE), LANE)].astype(F32)
            results.append(t[0:1] * above + t[1:2] * x + t[2:3] * below)
        gate, up = results
        hid[:, pl.ds(pl.multiple_of(n * LANE, LANE), LANE)] = (gate / (1.0 + jnp.exp(-gate)) * up).astype(BF16)
        return 0

    lax.fori_loop(0, half_w // LANE, conv, 0)
    advance(ADVANCE[9])

    right, left = {"tp": place.peer(1)}, {"tp": place.peer(peers - 1)}

    def sides(lo, hi):
        middle = (lo + hi) // 2
        first, second = pl.ds(lo * LANE, (middle - lo) * LANE), pl.ds(middle * LANE, (hi - middle) * LANE)
        return (0, first, second, right, place.peer(1)), (1, second, first, left, place.peer(peers - 1))

    def around_first(n, lo, hi):
        for plane, shared, alone, device, to in sides(lo, hi):
            far = ff.at[peer_rows(place.peer(2)), shared]
            remote(far, ff_r.at[2, :, shared], tp_s.at[2 + n], mid_r.at[n], device).start()
            near = ff.at[peer_rows(to), alone]
            remote(near, ff_r.at[plane, :, alone], tp_s.at[2 + n], tp_r.at[2 + n], device).start()

    def around_second(n, lo, hi):
        wait_bytes(ff_r.at[2, :, pl.ds(lo * LANE, (hi - lo) * LANE)], mid_r.at[n])
        for plane, shared, alone, device, to in sides(lo, hi):
            total = ff[peer_rows(to), shared].astype(F32) + ff_r[2, :, shared].astype(F32)
            pair_sum[plane, :, shared] = total.astype(BF16)
            remote(
                pair_sum.at[plane, :, shared], ff_r.at[plane, :, shared], tp_s.at[2 + n], tp_r.at[2 + n], device
            ).start()

    for part_no, (lo, hi) in enumerate(cuts):
        ready(down, part_no)

        def project_down(n, _):
            rows_ = pl.ds(pl.multiple_of(n * 2 * LANE, 2 * LANE), 2 * LANE)
            ff[:, rows_] = nt(hid[...], dn[rows_, :]).astype(BF16)
            return 0

        lax.fori_loop(lo // 2, hi // 2, project_down, 0)
        cols = pl.ds(lo * LANE, (hi - lo) * LANE)
        if AROUND and peers == 4:
            around_first(part_no, lo, hi)
        else:
            to_peers(
                lambda j: ff.at[peer_rows(j), cols],
                lambda step: ff_r.at[step - 1, :, cols],
                tp_s.at[2 + part_no],
                tp_r.at[2 + part_no],
            )
    if AROUND and peers == 4:
        for part_no, (lo, hi) in enumerate(cuts):
            around_second(part_no, lo, hi)
    for part_no, (lo, hi) in enumerate(cuts):
        cols = pl.ds(lo * LANE, (hi - lo) * LANE)
        arriving = 2 if AROUND and peers == 4 else peers - 1
        wait_bytes(ff_r.at[pl.ds(0, arriving), :, cols], tp_r.at[2 + part_no])
        for slot in range(lo, hi):
            held = pl.ds(slot * LANE, LANE)
            home = pl.ds(pl.multiple_of(place.slot_chip(slot) * LANE, LANE), LANE)
            total = ff[peer_rows(tp), held].astype(F32)
            for step in range(arriving):
                total = total + ff_r[step, :, held].astype(F32)
            out_ref[:, home] = (mid[:, home].astype(F32) + total).astype(BF16)
        for slot in range(lo, hi):
            home = pl.ds(pl.multiple_of(place.slot_chip(slot) * LANE, LANE), LANE)
            pltpu.make_async_copy(out_ref.at[:, home], out_hbm.at[:, home], out_sem).start()

    advance(10_000)
    for copy in halos + swaps + [handover]:
        copy.wait_send()
    for n in range(2):
        wait_bytes(att_r, tp_s.at[n])
    for n, (lo, hi) in enumerate(cuts):
        wait_bytes(ff_r.at[:, :, pl.ds(lo * LANE, (hi - lo) * LANE)], tp_s.at[2 + n])
    wait_bytes(st_send.at[others], a2a_s.at[0])
    wait_bytes(dec_recv.at[others], a2a_s.at[1])
    wait_bytes(in_send.at[others], a2a_s.at[2])
    gate_up.drain()
    down.drain()
    wait_bytes(out_ref, out_sem)


PAIRED = True
OWN_FIRST = 1
AROUND = False
GU_SHARE = 0.69
DOWN_SHARE = 0.66
RIM = 16
EARLY = 1
PAIR_LAG = 2
DOWN_LAG = 1
GU_PARTS = 2
DOWN_PARTS = 2
ADVANCE = (4, 7, 1, 5, 5, 2, 1, 1, 0, 1)


def solution(mesh):
    groups, spans, peers = mesh.shape["grp"], mesh.shape["sp"], mesh.shape["tp"]
    rows_, cols_ = ("grp", "sp"), "tp"
    placed = (
        P(rows_, cols_), P(rows_, cols_), P(rows_, cols_), P(rows_, cols_), P(None, cols_, rows_), P(None, cols_),
        P(cols_, None), P(rows_, None), P(), P("sp", cols_), P("sp", cols_), P("sp", cols_), P(None, cols_),
        P(None, cols_),
    )

    def shards(q, k, v, g, ld, hg, wo, res, ng, gw, uw, dw, gt, ut):
        length = q.shape[0]
        heads = q.shape[1] // HEAD
        combos = 2 * heads
        share = length // peers
        block, half_w = gw.shape
        width = wo.shape[1]
        chips = spans // 2
        packet = 2 * HEAD // chips
        dma = pltpu.SemaphoreType.DMA
        hbm = pl.BlockSpec(memory_space=pltpu.HBM)
        scratch = [pltpu.VMEM(a.shape, a.dtype) for a in (q, k, v, g, ld, hg, ng, gt, ut)] + [
            pltpu.VMEM((spans * block, 2 * half_w), BF16),
            pltpu.VMEM((spans * block, half_w), BF16),
            pltpu.VMEM(wo.shape, BF16),
            pltpu.VMEM((share, width), BF16),
            pltpu.VMEM((combos, HEAD, HEAD), BF16),
            pltpu.VMEM((combos, HEAD, HEAD), BF16),
            pltpu.VMEM((combos, 1, LANE), F32),
            pltpu.VMEM((combos, 1, LANE), F32),
            pltpu.VMEM((chips, packet, HEAD), BF16),
            pltpu.VMEM((chips, packet, HEAD), BF16),
            pltpu.VMEM((2, 1, LANE), F32),
            pltpu.VMEM((chips, 1, LANE), F32),
            pltpu.VMEM((chips, packet, HEAD), BF16),
            pltpu.VMEM((2, chips, packet, HEAD), BF16),
            pltpu.VMEM((chips, packet, HEAD), BF16),
            pltpu.VMEM((combos, length, HEAD), F32),
            pltpu.VMEM((combos, length, HEAD), F32),
            pltpu.VMEM((length, heads * HEAD), BF16),
            pltpu.VMEM((length, width), BF16),
            pltpu.VMEM((peers - 1, share, width), BF16),
            pltpu.VMEM((share, width), BF16),
            pltpu.VMEM((share, width), BF16),
            pltpu.VMEM((length, width), BF16),
            pltpu.VMEM((length + RIM, width), BF16),
            pltpu.VMEM((length + RIM, 2 * half_w), F32),
            pltpu.VMEM((2, 1, width), F32),
            pltpu.VMEM((2, 1, width), F32),
            pltpu.VMEM((length, half_w), BF16),
            pltpu.VMEM((length, width), BF16),
            pltpu.VMEM((peers - 1, share, width), BF16),
            pltpu.VMEM((2, share, width), BF16),
            pltpu.VMEM((share, width), BF16),
            dma((14,)), dma, dma((3,)), dma((3,)), dma((3,)), dma((3,)), dma((6,)), dma((6,)), dma((4,)), dma((2,)), dma((2,)),
        ]
        for parts, held in zip((GU_PARTS, DOWN_PARTS), groups_of(chips)):
            scratch += [dma((3,)), dma((chips, parts)), dma((chips // 2 + 1,)), dma((len(held),))]
        return pl.pallas_call(
            functools.partial(layer, groups, spans, peers),
            name="layer",
            out_shape=jax.ShapeDtypeStruct((share, width), BF16),
            in_specs=[hbm] * 14,
            out_specs=hbm,
            scratch_shapes=scratch,
            compiler_params=pltpu.CompilerParams(
                collective_id=0, has_side_effects=True, vmem_limit_bytes=67_043_328
            ),
        )(q, k, v, g, ld, hg, wo, res, ng, gw, uw, dw, gt, ut)

    return jax.shard_map(shards, mesh=mesh, in_specs=placed, out_specs=P(("grp", "sp", "tp"), None), check_vma=False)
```
